256 devices in a mesh: grp: 2 (over y), sp: 32 (over z, core), tp: 4 (over x).
Axes of the slice: x: 4, y: 2, z: 16, core: 2. Of those that a mesh axis runs over, the one named last changes fastest.
The devices are a block of a 4x16x16 slice.
Arguments:
- hidden_in: bfloat16 [16384, 2048], P(('grp', 'sp')), parts along dimension 0, may hold values from -6 to 6
- query_latent_rows: bfloat16 [16384, 768], P(('grp', 'sp')), parts along dimension 0, may hold values from -6 to 6
- key_value_latent: bfloat16 [16384, 512], P(('grp', 'sp')), parts along dimension 0, may hold values from -6 to 6
- rotary_key: bfloat16 [16384, 32], P(('grp', 'sp')), parts along dimension 0, may hold values from -64 to 64
- query_norm_gain: float32 [768], replicated, may hold values from 0.1 to 1.9
- key_value_gain: float32 [512], replicated, may hold values from 0.1 to 1.9
- query_up_weight: bfloat16 [768, 1536], P(None, 'tp'), may hold values from -0.625 to 0.625
- key_value_up_weight: bfloat16 [512, 2048], P(None, 'tp'), may hold values from -0.25 to 0.25
- out_proj: bfloat16 [1024, 2048], P('tp'), may hold values from -0.1875 to 0.1875
- feed_gain: float32 [2048], replicated, may hold values from 0.1 to 1.9
- feed_up: bfloat16 [2048, 8192], P('sp', 'tp'), may hold values from -0.125 to 0.125
- feed_down: bfloat16 [8192, 2048], P('tp', 'sp'), may hold values from -0.0625 to 0.0625
Outputs:
- layer_out: bfloat16 [16384, 2048], P(('grp', 'sp', 'tp')), parts along dimension 0
The draws below stay inside these ranges and needn't reach their ends.
There are 2 independent parts, one for each index of `grp`. The reference program is written for one: setup_inputs(seed, part) draws one part's arguments, and reference() takes and returns one part's arrays. A program takes and returns all parts, laid end to end along the dimension named above; an argument that names none is the same for every part. Nothing has to cross between parts.
All inputs are finite; a program needn't handle non-finite values.
Results may differ from the reference program's by a relative error of at most 0.02.
Values may be sent and summed in bfloat16 or wider, within the bound.
A program may use at most 128 MiB of HBM per device.

```python
import math
import jax
import jax.numpy as jnp
from jax import lax

D = 2048
HEAD_COUNT = 16
QUERY_KEY_PLAIN = 64
QUERY_KEY_ROTARY = 32
VALUE_HEAD_SIZE = 64
QUERY_RANK = 768
KEY_VALUE_RANK = 512
FF = 8192
TOKEN_COUNT = 8192


def draw_rotary_key(key, part):
    base = jax.random.normal(jax.random.fold_in(key, 11), (TOKEN_COUNT, QUERY_KEY_ROTARY), jnp.float32)
    return jnp.clip(base, -64.0, 64.0).astype(jnp.bfloat16)


def levels(stream_key, shape, shards, smallest, largest):
    level = 1.0
    for axis_at, blocks in shards:
        heights = jax.random.uniform(jax.random.fold_in(jax.random.fold_in(stream_key, 6), axis_at), (blocks,), jnp.float32, smallest / len(shards), largest / len(shards))
        level = level * jnp.repeat(jnp.exp(heights), shape[axis_at] // blocks).reshape((-1,) + (1,) * (len(shape) - 1 - axis_at))
    return level


def centred(stream_key, extent, deviation, limit, shards=(), kind=jnp.bfloat16):
    factor_of = levels(stream_key, extent, shards, -0.22, 0.18) if shards else 1.0
    drawn = jax.random.normal(stream_key, extent, jnp.float32) * deviation * factor_of
    return jnp.minimum(jnp.maximum(drawn, -limit), limit).astype(kind)


def setup_inputs(seed: int = 0, part: int = 0) -> dict:
    streams_of = jax.random.split(jax.random.key(seed), 13)
    part_keys = jax.random.split(jax.random.fold_in(streams_of[12], part), 13)
    hidden_in = centred(part_keys[0], (TOKEN_COUNT, D), 1.0, 6.0, ((0, 32),))
    query_latent_rows = centred(part_keys[1], (TOKEN_COUNT, QUERY_RANK), 1.0, 6.0, ((0, 32),))
    key_value_latent = centred(part_keys[2], (TOKEN_COUNT, KEY_VALUE_RANK), 1.0, 6.0, ((0, 32),))
    rotary_key = draw_rotary_key(jax.random.fold_in(jax.random.fold_in(streams_of[12], part), 71), part)
    query_norm_gain = jnp.clip(1.0 + 0.18 * jax.random.normal(streams_of[4], (QUERY_RANK,), jnp.float32), 0.1, 1.9)
    key_value_gain = jnp.clip(1.0 + 0.18 * jax.random.normal(streams_of[5], (KEY_VALUE_RANK,), jnp.float32), 0.1, 1.9)
    query_up_weight = centred(streams_of[6], (QUERY_RANK, HEAD_COUNT * (QUERY_KEY_PLAIN + QUERY_KEY_ROTARY)), (3 * QUERY_RANK ** -0.5), 0.625, ((1, 4),))
    key_value_up_weight = centred(streams_of[7], (KEY_VALUE_RANK, HEAD_COUNT * (QUERY_KEY_PLAIN + VALUE_HEAD_SIZE)), KEY_VALUE_RANK ** -0.5, 0.25, ((1, 4),))
    out_proj = centred(streams_of[8], (HEAD_COUNT * VALUE_HEAD_SIZE, D), (HEAD_COUNT * VALUE_HEAD_SIZE) ** -0.5, 0.1875, ((0, 4),))
    feed_gain = jnp.clip(1.0 + 0.18 * jax.random.normal(streams_of[9], (D,), jnp.float32), 0.1, 1.9)
    feed_up = centred(streams_of[10], (D, FF), D ** -0.5, 0.125, ((0, 32), (1, 4)))
    feed_down = centred(streams_of[11], (FF, D), FF ** -0.5, 0.0625, ((0, 4), (1, 32)))
    return {"hidden_in": hidden_in, "query_latent_rows": query_latent_rows, "key_value_latent": key_value_latent, "rotary_key": rotary_key, "query_norm_gain": query_norm_gain, "key_value_gain": key_value_gain, "query_up_weight": query_up_weight, "key_value_up_weight": key_value_up_weight, "out_proj": out_proj, "feed_gain": feed_gain, "feed_up": feed_up, "feed_down": feed_down}


def normalize(values, gain):
    floats = values.astype(jnp.float32)
    return floats * lax.rsqrt(lax.optimization_barrier(jnp.mean(floats * floats, axis=-1, keepdims=True)) + 1e-06) * gain.astype(jnp.float32)

def rotate(values, position):
    half_size = values.shape[-1] // 2
    inverse = 10000.0 ** (-jnp.arange(half_size, dtype=jnp.float32) * 2.0 / values.shape[-1])
    angles = position[:, None] * inverse[None, :]
    cosine = jnp.concatenate([jnp.cos(angles), jnp.cos(angles)], axis=-1)
    sine = jnp.concatenate([jnp.sin(angles), jnp.sin(angles)], axis=-1)
    shape = (values.shape[0],) + (1,) * (values.ndim - 2) + (values.shape[-1],)
    turned = jnp.concatenate([-values[..., half_size:], values[..., :half_size]], axis=-1)
    return values * cosine.reshape(shape) + turned * sine.reshape(shape)

def reference(hidden_in, query_latent_rows, key_value_latent, rotary_key, query_norm_gain, key_value_gain, query_up_weight, key_value_up_weight, out_proj, feed_gain, feed_up, feed_down):
    position = jnp.arange(TOKEN_COUNT).astype(jnp.float32)
    scale_factor = (QUERY_KEY_PLAIN + QUERY_KEY_ROTARY) ** (-0.5)
    query_norm = normalize(query_latent_rows, query_norm_gain).astype(jnp.bfloat16)
    queries = jnp.dot(query_norm, query_up_weight, preferred_element_type=jnp.float32).reshape(TOKEN_COUNT, HEAD_COUNT, QUERY_KEY_PLAIN + QUERY_KEY_ROTARY)
    queries = jnp.concatenate([queries[..., :QUERY_KEY_PLAIN], rotate(queries[..., QUERY_KEY_PLAIN:], position)], axis=-1).astype(jnp.bfloat16)
    latent = normalize(key_value_latent, key_value_gain).astype(jnp.bfloat16)
    keys_values = jnp.dot(latent, key_value_up_weight, preferred_element_type=jnp.float32).astype(jnp.bfloat16)
    keys_values = keys_values.reshape(TOKEN_COUNT, HEAD_COUNT, QUERY_KEY_PLAIN + VALUE_HEAD_SIZE)
    key_nope = keys_values[..., :QUERY_KEY_PLAIN].astype(jnp.float32)
    value_rows = keys_values[..., QUERY_KEY_PLAIN:].astype(jnp.float32)
    key_rope = rotate(rotary_key.astype(jnp.float32), position).astype(jnp.bfloat16).astype(jnp.float32)
    block = math.gcd(TOKEN_COUNT, 512)
    query_blocks = queries.reshape(TOKEN_COUNT // block, block, HEAD_COUNT, QUERY_KEY_PLAIN + QUERY_KEY_ROTARY)

    def attend(query_block):
        plain = query_block[..., :QUERY_KEY_PLAIN].astype(jnp.float32)
        turned = query_block[..., QUERY_KEY_PLAIN:].astype(jnp.float32)
        scores = jnp.einsum('qhd,khd->hqk', plain, key_nope) + jnp.einsum('qhd,kd->hqk', turned, key_rope)
        scores = scores * scale_factor
        expo = jnp.exp(scores - lax.optimization_barrier(jnp.max(scores, axis=-1, keepdims=True)))
        total = lax.optimization_barrier(jnp.sum(expo, axis=-1))
        weights = expo.astype(jnp.bfloat16).astype(jnp.float32)
        summed = jnp.einsum('hqk,khd->qhd', weights, value_rows)
        return summed / jnp.transpose(total)[:, :, None]
    mixed = lax.map(attend, query_blocks).reshape(TOKEN_COUNT, HEAD_COUNT * VALUE_HEAD_SIZE).astype(jnp.bfloat16)
    branch = jnp.dot(mixed, out_proj, preferred_element_type=jnp.float32)
    middle = (hidden_in.astype(jnp.float32) + branch).astype(jnp.bfloat16)
    normed = normalize(middle, feed_gain).astype(jnp.bfloat16)
    upward = jnp.dot(normed, feed_up, preferred_element_type=jnp.float32)
    activated = jnp.square(jax.nn.relu(upward)).astype(jnp.bfloat16)
    feed = jnp.dot(activated, feed_down, preferred_element_type=jnp.float32)
    return (middle.astype(jnp.float32) + feed).astype(jnp.bfloat16)
```

```python
import functools
import math

import jax
import jax.numpy as jnp
from jax import lax
from jax.experimental import pallas as pl
from jax.experimental.pallas import tpu as pltpu
from jax.sharding import PartitionSpec as P

PLAIN = 64
ROTARY = 32
VALUE = 64
MESH = pl.DeviceIdType.MESH
LANES = 128
SUB = 2


def normalize(values, gain):
    floats = values.astype(jnp.float32)
    return floats * lax.rsqrt(jnp.mean(floats * floats, axis=-1, keepdims=True) + 1e-06) * gain


def nt_dot(a, b):
    return lax.dot_general(a, b, (((1,), (1,)), ((), ())), preferred_element_type=jnp.float32)


def layer_kernel(
    Z, X,
    x_own, up_own, dn_own, hid, qp, qr, wk, wvt, wo, gain,
    out,
    xb, U, D, hrow, q2t, s_buf, vt, m_sc, l_sc, o_sc, mixed, bsend, brecv, mid, nb, act, osend, orecv,
    loc_s, lz_s, lz_r, lx1_s, lx1_r, lx2_s, lx2_r, ld_s, ld_r, wz_s, wz_r, wd_s, wd_r, wo_s, wo_r,
    rs_s, rs_r, ag_s, ag_r, fo_s, fo_r,
):
    HALF = Z // 2
    NT = SUB * HALF
    sp = lax.axis_index("sp")
    x = lax.axis_index("tp")
    z = sp // 2
    c = sp % 2
    sgn = 1 - 2 * c
    T = nb.shape[0]
    share = T // X
    shard = up_own.shape[0]
    srow = shard // SUB
    KB = wk.shape[0] // LANES
    qrows = x_own.shape[1]
    gsub = LANES // ROTARY
    grow = share // gsub
    keys = 4 * T
    gkeys = keys // gsub
    F = U.shape[1]
    W = U.shape[0]

    def at(zz):
        return lax.rem(zz + 2 * Z, Z)

    def zdev(zz):
        return {"sp": 2 * at(zz) + c}

    sib = {"sp": 2 * z + 1 - c}

    def xdev(d):
        return {"tp": lax.rem(x + d + X, X)}

    def rcopy(src, dst, ss, rs, dev):
        return pltpu.make_async_remote_copy(
            src_ref=src, dst_ref=dst, send_sem=ss, recv_sem=rs, device_id=dev, device_id_type=MESH
        )

    def zside(side, t):
        return at(z - t) if side == 0 else at(z + t)

    mine = x * share
    loads = [
        pltpu.make_async_copy(x_own, xb.at[z, c], loc_s.at[0]),
        pltpu.make_async_copy(up_own, U.at[pl.ds(pl.multiple_of(z * 2 * shard + c * shard, 32), shard)], loc_s.at[1]),
        pltpu.make_async_copy(dn_own, D.at[pl.ds(pl.multiple_of(z * 2 * shard + c * shard, 32), shard)], loc_s.at[2]),
        pltpu.make_async_copy(hid.at[pl.ds(pl.multiple_of(mine, share), share)], hrow, loc_s.at[3]),
    ]
    for load in loads:
        load.start()
    barrier = pltpu.get_barrier_semaphore()
    peers = [zdev(z + 1), zdev(z - 1), sib] + [xdev(d) for d in range(1, X)]
    for dev in peers:
        pl.semaphore_signal(barrier, inc=1, device_id=dev, device_id_type=MESH)
    pl.semaphore_wait(barrier, len(peers))
    for load in loads:
        load.wait()

    def lat(zz, core):
        return xb.at[zz, core, x]

    def lz_send(zz, side, hop, dev):
        rcopy(lat(zz, c), lat(zz, c), lz_s.at[side, hop], lz_r.at[side, hop], dev).start()

    def lz_wait(side, hop):
        rcopy(lat(z, c), lat(z, c), lz_s.at[side, hop], lz_r.at[side, hop], zdev(z + 1)).wait_recv()

    half_rows = qrows // 2
    def x1_send(zz, side, t):
        for i, d in enumerate((1, -1)):
            rcopy(xb.at[zz, c, x], xb.at[zz, c, x], lx1_s.at[i, side, t], lx1_r.at[i, side, t], xdev(d)).start()

    def x1_wait(side, t):
        for i, d in enumerate((1, -1)):
            rcopy(xb.at[z, c, x], xb.at[z, c, x], lx1_s.at[i, side, t], lx1_r.at[i, side, t], xdev(d)).wait_recv()

    def x2_part(zz, q, i):
        return xb.at[zz, c, q, pl.ds(i * 128, 128 if i == 0 else qrows - 128)]

    def x2_send(zz, side, t):
        for i, d in enumerate((1, -1)):
            part = x2_part(zz, lax.rem(x - d + X, X), i)
            rcopy(part, part, lx2_s.at[i, side, t], lx2_r.at[i, side, t], xdev(d)).start()

    def x2_wait(side, t):
        for i, d in enumerate((1, -1)):
            part = x2_part(z, x, i)
            rcopy(part, part, lx2_s.at[i, side, t], lx2_r.at[i, side, t], xdev(d)).wait_recv()

    def ld_send(zz, side, t):
        rcopy(xb.at[zz, c], xb.at[zz, c], ld_s.at[side, t], ld_r.at[side, t], sib).start()

    def ld_wait(side, t):
        rcopy(xb.at[z, c], xb.at[z, c], ld_s.at[side, t], ld_r.at[side, t], sib).wait_recv()

    weights = (U, D)

    def wslice(arr, zz, core, s):
        start = pl.multiple_of(zz * (2 * shard) + core * shard + s * srow, srow)
        return weights[arr].at[pl.ds(start, srow)]

    def wz_copy(arr, zz, side, k, dev):
        piece = wslice(arr, zz, c, lax.rem(k, SUB))
        return rcopy(piece, piece, wz_s.at[arr, side, k], wz_r.at[arr, side, k], dev)

    def wd_copy(arr, zz, side, k):
        piece = wslice(arr, zz, c, lax.rem(k, SUB))
        return rcopy(piece, piece, wd_s.at[arr, side, k], wd_r.at[arr, side, k], sib)

    def own_copy(arr):
        start = pl.multiple_of(z * 2 * shard + c * shard, shard)
        piece = weights[arr].at[pl.ds(start, shard)]
        return rcopy(piece, piece, wo_s.at[arr], wo_r.at[arr], sib)

    def w_first(arr):
        for k in range(SUB):
            if HALF > 1:
                wz_copy(arr, z, 0, jnp.int32(k), zdev(z + 1)).start()
                wz_copy(arr, z, 1, jnp.int32(k), zdev(z - 1)).start()
        own_copy(arr).start()

    def w_serve(arr, k):
        k = jnp.int32(k)
        hop = k // SUB + 1

        @pl.when(hop < HALF)
        def _():
            for side in range(2):
                wz_copy(arr, z, side, k, zdev(z + 1)).wait_recv()

        @pl.when(hop < HALF - 1)
        def _():
            wz_copy(arr, at(z - hop), 0, k + SUB, zdev(z + 1)).start()
            wz_copy(arr, at(z + hop), 1, k + SUB, zdev(z - 1)).start()

        @pl.when(hop == HALF - 1)
        def _():
            wz_copy(arr, at(z - hop * sgn), 0, k + SUB, zdev(z + sgn)).start()

        @pl.when(hop < HALF)
        def _():
            for side in range(2):
                wd_copy(arr, zside(side, hop), side, k).start()

        @pl.when(hop == HALF)
        def _():
            wz_copy(arr, z, 0, k, zdev(z + 1)).wait_recv()
            wd_copy(arr, at(z + HALF), 0, k).start()

    lz_send(z, 0, 1, zdev(z + 1))
    lz_send(z, 1, 1, zdev(z - 1))
    w_first(0)
    ld_send(z, 0, 0)

    tok = qp.shape[1]
    q2t[...] = jnp.zeros_like(q2t)
    for g in range(gsub):
        for p in range(2):
            for hh in range(2):
                h = 2 * p + hh
                q2t[g, p, hh * PLAIN:(hh + 1) * PLAIN, hh * tok:(hh + 1) * tok] = qp[h * PLAIN:(h + 1) * PLAIN, :]
                q2t[g, p, LANES + g * ROTARY:LANES + (g + 1) * ROTARY, hh * tok:(hh + 1) * tok] = (
                    qr[h * ROTARY:(h + 1) * ROTARY, :]
                )
    m_sc[...] = jnp.full_like(m_sc, -1e30)
    l_sc[...] = jnp.zeros_like(l_sc)
    o_sc[...] = jnp.zeros_like(o_sc)

    def attend(za, zb):
        for g in range(gsub):
            def rows(first, count):
                return jnp.concatenate(
                    [xb[zz, :, :, first:first + count, :].reshape(gkeys // 2, LANES) for zz in (za, zb)], axis=0
                )
            lhs = jnp.concatenate([rows(kb * share + g * grow, grow) for kb in range(KB)], axis=1)
            rope = rows(KB * share, grow)
            kk = jnp.dot(lhs, wk[...], preferred_element_type=jnp.float32).astype(jnp.bfloat16)
            vt[:, g * gkeys:(g + 1) * gkeys] = nt_dot(wvt[...], lhs).astype(jnp.bfloat16)
            for p in range(2):
                k2 = jnp.concatenate([kk[:, p * LANES:(p + 1) * LANES], rope], axis=1)
                s_buf[p, g * gkeys:(g + 1) * gkeys, :] = jnp.dot(
                    k2, q2t[g, p], preferred_element_type=jnp.float32
                )
        for p in range(2):
            old = m_sc[p:p + 1, :]
            new = jnp.maximum(old, jnp.max(s_buf[p], axis=0, keepdims=True))
            factor = jnp.exp2(old - new)
            m_sc[p:p + 1, :] = new
            expo = jnp.exp2(s_buf[p] - new)
            l_sc[p:p + 1, :] = l_sc[p:p + 1, :] * factor + jnp.sum(expo, axis=0, keepdims=True)
            weights_t = expo.astype(jnp.bfloat16)
            for hh in range(2):
                h = 2 * p + hh
                lanes = slice(hh * tok, (hh + 1) * tok)
                o_sc[h] = o_sc[h] * factor[:, lanes] + jnp.dot(
                    vt[h * VALUE:(h + 1) * VALUE, :], weights_t[:, lanes], preferred_element_type=jnp.float32
                )

    SKEW = 2

    def phase(i, carry):
        @pl.when(i < HALF)
        def _():
            for side in range(2):
                lz_wait(side, i)

        @pl.when(i < HALF - 1)
        def _():
            lz_send(at(z - i), 0, i + 1, zdev(z + 1))
            lz_send(at(z + i), 1, i + 1, zdev(z - 1))

        @pl.when(i == HALF - 1)
        def _():
            lz_send(at(z - i * sgn), 0, i + 1, zdev(z + sgn))

        @pl.when(i < HALF)
        def _():
            for side in range(2):
                x1_send(zside(side, i), side, i)

        @pl.when(i == HALF)
        def _():
            lz_wait(0, i)
            x1_send(at(z + HALF), 0, i)

        w_serve(0, i - 1)
        j = i - 1

        @pl.when((j >= 1) & (j < HALF))
        def _():
            for side in range(2):
                x1_wait(side, j)
            for side in range(2):
                x2_send(zside(side, j), side, j)

        @pl.when(j == HALF)
        def _():
            x1_wait(0, j)
            x2_send(at(z + HALF), 0, j)

        @pl.when(i > SKEW)
        def _():
            t = i - SKEW

            @pl.when(t < HALF)
            def _():
                for side in range(2):
                    ld_wait(side, t)

            @pl.when(t == HALF)
            def _():
                ld_wait(0, t)
                ld_wait(0, 0)

            attend(at(z - lax.rem(t, HALF)), at(z + t))

        @pl.when((j >= 1) & (j < HALF))
        def _():
            for side in range(2):
                x2_wait(side, j)
                ld_send(zside(side, j), side, j)

        @pl.when(j == HALF)
        def _():
            x2_wait(0, j)
            ld_send(at(z + HALF), 0, j)

        return carry

    lax.fori_loop(1, HALF + SKEW + 1, phase, 0)

    served = [HALF + SKEW]
    begun = [False]

    def serve_upto(n):
        while served[0] < min(n, 2 * NT):
            k = served[0]
            if k >= NT - 2 * SUB and not begun[0]:
                w_first(1)
                begun[0] = True
            w_serve(k // NT, k % NT)
            served[0] += 1

    heads = []
    for h in range(4):
        p, hh = h // 2, h % 2
        heads.append(o_sc[h] / l_sc[p:p + 1, hh * tok:(hh + 1) * tok])
    mixed[...] = jnp.transpose(jnp.concatenate(heads, axis=0)).astype(jnp.bfloat16)
    NB = 256
    def project(n, carry):
        cols = pl.ds(pl.multiple_of(n * NB, NB), NB)
        bsend[:, cols] = jnp.dot(mixed[...], wo[:, cols], preferred_element_type=jnp.float32).astype(jnp.bfloat16)
        return carry
    lax.fori_loop(0, W // NB, project, 0)

    def rowsof(q):
        return pl.ds(pl.multiple_of(q * share, share), share)

    branch = []
    for d in range(1, X):
        q = lax.rem(x + d, X)
        branch.append(rcopy(bsend.at[rowsof(q)], brecv.at[d - 1], rs_s.at[d - 1], rs_r.at[d - 1], xdev(d)))
        branch[-1].start()
    serve_upto(NT - 2)
    total = bsend[rowsof(x), :].astype(jnp.float32)
    for copy in branch:
        copy.wait_recv()
    for d in range(X - 1):
        total = total + brecv[d].astype(jnp.float32)
    middle = (hrow[...].astype(jnp.float32) + total).astype(jnp.bfloat16)
    mid[...] = middle
    nb[rowsof(x), :] = normalize(middle, gain[...]).astype(jnp.bfloat16)
    spread = []
    for d in range(1, X):
        spread.append(rcopy(nb.at[rowsof(x)], nb.at[rowsof(x)], ag_s.at[d - 1], ag_r.at[d - 1], xdev(d)))
        spread[-1].start()
    serve_upto(NT + 2)
    for copy in spread:
        copy.wait_recv()

    def wd_wait(arr, k):
        hop = k // SUB + 1
        for side in range(2 if hop < HALF else 1):
            wd_copy(arr, z, side, jnp.int32(k)).wait_recv()

    own_copy(0).wait_recv()
    for k in range(NT):
        wd_wait(0, k)
    CUTS = 4
    per = F // NB // CUTS
    for cut in range(CUTS):
        def up(n, carry):
            cols = pl.ds(pl.multiple_of(n * NB, NB), NB)
            high = jnp.maximum(jnp.dot(nb[...], U[:, cols], preferred_element_type=jnp.float32), 0.0)
            act[:, cols] = (high * high).astype(jnp.bfloat16)
            return carry
        lax.fori_loop(cut * per, (cut + 1) * per, up, 0)
        if cut < CUTS - 1:
            serve_upto(NT + 3 + cut)

    def fo_copy(t, d):
        q = lax.rem(x + d, X)
        return rcopy(osend.at[t, q], orecv.at[t, d - 1], fo_s.at[t, d - 1], fo_r.at[t, d - 1], xdev(d))

    def pair_of(t):
        return at(z - (t % HALF)), at(z + t)

    for t in range(1, HALF + 1):
        serve_upto(NT + 2 * t)
        if t == HALF:
            own_copy(1).wait_recv()
        for k in (2 * t - 2, 2 * t - 1):
            wd_wait(1, k)
        rhs = jnp.concatenate(
            [D[pl.ds(pl.multiple_of(zz * 2 * shard, 2 * shard), 2 * shard), :] for zz in pair_of(t)], axis=0
        )
        block = nt_dot(act[...], rhs).astype(jnp.bfloat16)
        for q in range(X):
            for side in range(2):
                osend[t - 1, q, side] = block[q * share:(q + 1) * share, side * LANES:(side + 1) * LANES]
        for d in range(1, X):
            fo_copy(t - 1, d).start()
    for t in range(1, HALF + 1):
        for d in range(1, X):
            fo_copy(t - 1, d).wait_recv()
        for side, zz in enumerate(pair_of(t)):
            cols = pl.ds(pl.multiple_of(zz * LANES, LANES), LANES)
            total = osend[t - 1, x, side].astype(jnp.float32)
            for d in range(X - 1):
                total = total + orecv[t - 1, d, side].astype(jnp.float32)
            out[:, cols] = (mid[:, cols].astype(jnp.float32) + total).astype(jnp.bfloat16)

    for copy in branch + spread:
        copy.wait_send()
    for t in range(HALF):
        for d in range(1, X):
            fo_copy(t, d).wait_send()
    ld_wait_s = lambda side, t: rcopy(xb.at[z, c], xb.at[z, c], ld_s.at[side, t], ld_r.at[side, t], sib).wait_send()
    ld_wait_s(0, 0)
    for arr in range(2):
        own_copy(arr).wait_send()

    def drain(t, carry):
        def both(side):
            rcopy(lat(z, c), lat(z, c), lz_s.at[side, t], lz_r.at[side, t], zdev(z + 1)).wait_send()
            for i, d in enumerate((1, -1)):
                rcopy(xb.at[z, c, x], xb.at[z, c, x], lx1_s.at[i, side, t], lx1_r.at[i, side, t], xdev(d)).wait_send()
                part = x2_part(z, x, i)
                rcopy(part, part, lx2_s.at[i, side, t], lx2_r.at[i, side, t], xdev(d)).wait_send()
            ld_wait_s(side, t)
            for arr in range(2):
                for s in range(SUB):
                    k = (t - 1) * SUB + s
                    wz_copy(arr, z, side, k, zdev(z + 1)).wait_send()
                    wd_copy(arr, z, side, k).wait_send()
        both(0)
        pl.when(t < HALF)(lambda: both(1))
        return carry
    lax.fori_loop(1, HALF + 1, drain, 0)


def fused_layer(Z, X, x_own, up_own, dn_own, hid, qp, qr, wk, wvt, wo, gain, F):
    HALF = Z // 2
    NT = SUB * HALF
    T, W = hid.shape
    share = T // X
    bf, f32 = jnp.bfloat16, jnp.float32
    DMA = pltpu.SemaphoreType.DMA
    any_ = pl.BlockSpec(memory_space=pl.ANY)
    vm = pl.BlockSpec(memory_space=pltpu.VMEM)
    scratch = [
        pltpu.VMEM((Z, 2) + x_own.shape, bf),
        pltpu.VMEM((W, F), bf),
        pltpu.VMEM((W, F), bf),
        pltpu.VMEM((share, W), bf),
        pltpu.VMEM((LANES // ROTARY, 2, 2 * LANES, 2 * T), bf),
        pltpu.VMEM((2, 4 * T, 2 * T), f32),
        pltpu.VMEM((wvt.shape[0], 4 * T), bf),
        pltpu.VMEM((2, 2 * T), f32),
        pltpu.VMEM((2, 2 * T), f32),
        pltpu.VMEM((4, VALUE, T), f32),
        pltpu.VMEM((T, 4 * VALUE), bf),
        pltpu.VMEM((T, W), bf),
        pltpu.VMEM((X - 1, share, W), bf),
        pltpu.VMEM((share, W), bf),
        pltpu.VMEM((T, W), bf),
        pltpu.VMEM((T, F), bf),
        pltpu.VMEM((HALF, X, 2, share, LANES), bf),
        pltpu.VMEM((HALF, X - 1, 2, share, LANES), bf),
        DMA((4,)),
        DMA((2, HALF + 1)), DMA((2, HALF + 1)),
        DMA((2, 2, HALF + 1)), DMA((2, 2, HALF + 1)),
        DMA((2, 2, HALF + 1)), DMA((2, 2, HALF + 1)),
        DMA((2, HALF + 1)), DMA((2, HALF + 1)),
        DMA((2, 2, NT)), DMA((2, 2, NT)),
        DMA((2, 2, NT)), DMA((2, 2, NT)),
        DMA((2,)), DMA((2,)),
        DMA((X - 1,)), DMA((X - 1,)),
        DMA((X - 1,)), DMA((X - 1,)),
        DMA((HALF, X - 1)), DMA((HALF, X - 1)),
    ]
    return pl.pallas_call(
        functools.partial(layer_kernel, Z, X),
        out_shape=jax.ShapeDtypeStruct((share, W), bf),
        in_specs=[any_, any_, any_, any_, vm, vm, vm, vm, vm, vm],
        out_specs=vm,
        scratch_shapes=scratch,
        compiler_params=pltpu.CompilerParams(
            collective_id=0, has_side_effects=True, vmem_limit_bytes=62 * 1024 * 1024
        ),
        name="layer",
    )(x_own, up_own, dn_own, hid, qp, qr, wk, wvt, wo, gain)


def on_device(
    hidden_in, query_latent_rows, key_value_latent, rotary_key, query_norm_gain, key_value_gain,
    query_up_weight, key_value_up_weight, out_proj, feed_gain, feed_up, feed_down,
):
    X = lax.axis_size("tp")
    Z = lax.axis_size("sp") // 2
    T = hidden_in.shape[0]
    heads = query_up_weight.shape[1] // (PLAIN + ROTARY)
    share = T // X
    half = ROTARY // 2
    position = (lax.axis_index("sp") * T + jnp.arange(T)).astype(jnp.float32)
    inverse = 10000.0 ** (-jnp.arange(half, dtype=jnp.float32) * 2.0 / ROTARY)
    angles = position[:, None] * inverse[None, :]
    cosine, sine = jnp.cos(angles), jnp.sin(angles)
    scale = (PLAIN + ROTARY) ** (-0.5) * math.log2(math.e)

    query_norm = normalize(query_latent_rows, query_norm_gain).astype(jnp.bfloat16)
    queries = jnp.dot(query_norm, query_up_weight, preferred_element_type=jnp.float32)
    queries = queries.reshape(T, heads, PLAIN + ROTARY) * scale
    first, second = queries[..., PLAIN:PLAIN + half], queries[..., PLAIN + half:]
    cq, sq = cosine[:, None, :], sine[:, None, :]
    turned = jnp.concatenate([first * cq - second * sq, second * cq + first * sq], axis=-1)
    qp = queries[..., :PLAIN].astype(jnp.bfloat16).reshape(T, heads * PLAIN).T
    qr = turned.astype(jnp.bfloat16).reshape(T, heads * ROTARY).T

    latent = normalize(key_value_latent, key_value_gain).astype(jnp.bfloat16)
    key = rotary_key.astype(jnp.float32)
    k1, k2 = key[:, :half], key[:, half:]
    key_rope = jnp.concatenate([k1 * cosine - k2 * sine, k2 * cosine + k1 * sine], axis=-1).astype(jnp.bfloat16)
    KB = latent.shape[1] // LANES
    groups = LANES // ROTARY
    packed = latent.reshape(X, share, KB, LANES).transpose(0, 2, 1, 3).reshape(X, KB * share, LANES)
    ropes = key_rope.reshape(X, groups, share // groups, ROTARY).transpose(0, 2, 1, 3)
    x_own = jnp.concatenate([packed, ropes.reshape(X, share // groups, LANES)], axis=1)

    both = key_value_up_weight.reshape(-1, heads, PLAIN + VALUE)
    wk = both[..., :PLAIN].reshape(-1, heads * PLAIN)
    wvt = both[..., PLAIN:].reshape(-1, heads * VALUE).T
    return fused_layer(
        Z, X, x_own, feed_up, feed_down.T, hidden_in, qp, qr, wk, wvt, out_proj,
        feed_gain.reshape(1, -1), feed_up.shape[1],
    )


def solution(mesh):
    return jax.shard_map(
        on_device,
        mesh=mesh,
        in_specs=(
            P(("grp", "sp"), None),
            P(("grp", "sp"), None),
            P(("grp", "sp"), None),
            P(("grp", "sp"), None),
            P(),
            P(),
            P(None, "tp"),
            P(None, "tp"),
            P("tp", None),
            P(),
            P("sp", "tp"),
            P("tp", "sp"),
        ),
        out_specs=P(("grp", "sp", "tp"), None),
        check_vma=False,
    )
```

```python
import functools
import math

import jax
import jax.numpy as jnp
from jax import lax
from jax.experimental import pallas as pl
from jax.experimental.pallas import tpu as pltpu
from jax.sharding import PartitionSpec as P

PLAIN = 64
ROTARY = 32
VALUE = 64
MESH = pl.DeviceIdType.MESH
LANES = 128


def normalize(values, gain_ref):
    floats = values.astype(jnp.float32)
    inverse = lax.rsqrt(jnp.mean(floats * floats, axis=-1, keepdims=True) + 1e-06)
    return jnp.concatenate(
        [
            floats[:, k * LANES:(k + 1) * LANES] * inverse * gain_ref[k:k + 1, :]
            for k in range(values.shape[1] // LANES)
        ],
        axis=1,
    ).astype(jnp.bfloat16)


def nt_dot(a, b):
    return lax.dot_general(a, b, (((1,), (1,)), ((), ())), preferred_element_type=jnp.float32)


def layer_kernel(
    Z, X, paired,
    kvl, key_t, up_own, dn_own, hid, ql, wq, wkv, wo, cos_t, sin_t, q_gain, kv_gain, gain,
    out,
    xb, turned_key, U, D, hrow, WKV, WO, qx, q2t, wk, wvt, s_buf, m_sc, l_sc, o_sc, obuf, orx, relay, lse, wts, msend, mixed,
    mid, nb, act, osend, orecv, opart, ofar,
    loc_s, lz_s, lz_r, ld_s, ld_r, wz_s, wz_r, wy_s, wy_r, wd_s, wd_r, yd_s, yd_r, wo_s, wo_r,
    x1_s, x1_r, x2_s, x2_r, xd_s, xd_r, ml_s, ml_r, mo_s, mo_r, mh_s, mh_r, mr_s, mr_r, md_s, md_r,
    ag_s, ag_r, ah_s, ah_r, fa_s, fa_r, fo_s, fo_r, fz_s, fz_r,
):
    HALF = Z // 2
    sp = lax.axis_index("sp")
    x = lax.axis_index("tp")
    z = sp // 2
    c = sp % 2
    sgn = 1 - 2 * c
    group = lax.axis_index("grp")
    par = group % 2
    T, W = nb.shape
    F = U.shape[1]
    share = T // X
    shard = up_own.shape[0]
    KB = kvl.shape[1] // LANES
    gsub = LANES // ROTARY
    grow = share // gsub
    HP = wkv.shape[1] // (PLAIN + VALUE)
    HC = HP * X // 2
    bf = jnp.bfloat16
    f32 = jnp.float32

    def at(zz):
        return lax.rem(zz + 2 * Z, Z)

    def zdev(zz):
        return {"sp": 2 * at(zz) + c}

    sib = {"sp": 2 * z + 1 - c}
    twin = {"grp": group + 1 - 2 * par}

    def xat(d):
        return lax.rem(x + d + X, X)

    def xdev(d):
        return {"tp": xat(d)}

    def rcopy(src, dst, ss, rs, dev):
        return pltpu.make_async_remote_copy(
            src_ref=src, dst_ref=dst, send_sem=ss, recv_sem=rs, device_id=dev, device_id_type=MESH
        )

    def zside(side, t):
        return at(z - t) if side == 0 else at(z + t)

    def shard_at(zz, core):
        return pl.multiple_of(zz * (2 * shard) + core * shard, shard)

    def rowsof(q):
        return pl.ds(pl.multiple_of(q * share, share), share)

    loads = [
        pltpu.make_async_copy(wkv, WKV.at[x], loc_s.at[0]),
        pltpu.make_async_copy(up_own, U.at[pl.ds(shard_at(z, c), shard)], loc_s.at[1]),
        pltpu.make_async_copy(wo, WO.at[x], loc_s.at[2]),
        pltpu.make_async_copy(hid.at[rowsof(x)], hrow, loc_s.at[3]),
        pltpu.make_async_copy(dn_own, D.at[pl.ds(shard_at(z, c), shard)], loc_s.at[4]),
    ]
    for load in loads:
        load.start()
    barrier = pltpu.get_barrier_semaphore()
    peers = [zdev(z + 1), zdev(z - 1), sib] + [xdev(d) for d in range(1, X)] + ([twin] if paired else [])
    for dev in peers:
        pl.semaphore_signal(barrier, inc=1, device_id=dev, device_id_type=MESH)

    latent = normalize(kvl[rowsof(x), :], kv_gain)
    for kb in range(KB):
        xb[z, c, kb * share:(kb + 1) * share, :] = latent[:, kb * LANES:(kb + 1) * LANES]
    cosine, sine = cos_t[...], sin_t[...]
    half = ROTARY // 2
    key_first = key_t[0:half, :].astype(f32)
    key_second = key_t[half:ROTARY, :].astype(f32)
    turned_key[...] = jnp.transpose(
        jnp.concatenate(
            [
                key_first * cosine - key_second * sine,
                key_second * cosine + key_first * sine,
                jnp.zeros((LANES - ROTARY, T), f32),
            ],
            axis=0,
        )
    )
    packed_key = 0.0
    for g in range(gsub):
        piece = turned_key[pl.ds(pl.multiple_of(x * share + g * grow, grow), grow), :]
        packed_key = packed_key + (piece if g == 0 else pltpu.roll(piece, g * ROTARY, 1))
    xb[z, c, KB * share:, :] = packed_key.astype(bf)
    pl.semaphore_wait(barrier, len(peers))

    def lz_copy(zz, side, hop, dev):
        piece = xb.at[zz, c]
        return rcopy(piece, piece, lz_s.at[side, hop], lz_r.at[side, hop], dev)

    def ld_copy(zz, side, t):
        return rcopy(xb.at[zz, c], xb.at[zz, c], ld_s.at[side, t], ld_r.at[side, t], sib)

    def lz_step(i):
        i = jnp.int32(i)

        @pl.when(i < HALF)
        def _():
            for side in range(2):
                lz_copy(z, side, i, zdev(z + 1)).wait_recv()

        @pl.when(i < HALF - 1)
        def _():
            lz_copy(at(z - i), 0, i + 1, zdev(z + 1)).start()
            lz_copy(at(z + i), 1, i + 1, zdev(z - 1)).start()

        @pl.when(i == HALF - 1)
        def _():
            lz_copy(at(z - i * sgn), 0, i + 1, zdev(z + sgn)).start()

        @pl.when(i < HALF)
        def _():
            for side in range(2):
                ld_copy(zside(side, i), side, i).start()

        @pl.when(i == HALF)
        def _():
            lz_copy(z, 0, i, zdev(z + 1)).wait_recv()
            ld_copy(at(z + HALF), 0, i).start()

    kv_half, q_half, o_half = WKV.shape[1] // 2, qx.shape[2], WO.shape[1] // 2

    def x_piece(what, q, lo=0, parts=1):
        if what == 0:
            n = kv_half // parts
            return WKV.at[q, pl.ds(pl.multiple_of(c * kv_half + lo * n, n), n)]
        if what == 1:
            n = q_half // parts
            return qx.at[q, c, pl.ds(lo * n, n)]
        n = o_half // parts
        return WO.at[q, pl.ds(pl.multiple_of(c * o_half + lo * n, n), n)]

    def x1_copy(what, i, d):
        piece = x_piece(what, x)
        return rcopy(piece, piece, x1_s.at[what, i], x1_r.at[what, i], xdev(d))

    def x2_copy(what, i, d):
        piece = x_piece(what, xat(-d), i, 2)
        return rcopy(piece, piece, x2_s.at[what, i], x2_r.at[what, i], xdev(d))

    def xd_copy(what, n):
        if what == 2:
            piece = x_piece(2, xat(n + 1))
        else:
            piece = x_piece(what, (1 - c) * (X // 2) + n)
        return rcopy(piece, piece, xd_s.at[what, n], xd_r.at[what, n], sib)

    def x_first(what):
        for i, d in enumerate((1, -1)):
            x1_copy(what, i, d).start()

    def x_relay(what):
        for i, d in enumerate((1, -1)):
            x1_copy(what, i, d).wait_recv()
            x2_copy(what, i, d).start()

    def x_share(what):
        for i, d in enumerate((1, -1)):
            x2_copy(what, i, d).wait_recv()
        for n in range(X - 1 if what == 2 else X // 2):
            if what == 0:
                pl.when((1 - c) * (X // 2) + n != x)(lambda: xd_copy(0, n).start())
            else:
                xd_copy(what, n).start()

    def x_end(what):
        for n in range(X - 1 if what == 2 else X // 2):
            if what == 0:
                pl.when(c * (X // 2) + n != x)(lambda: xd_copy(0, n).wait_recv())
            else:
                xd_copy(what, n).wait_recv()

    weights = (U, D)
    ZW = 3 if paired else 4
    part = shard // 4
    NP = ZW * HALF

    def place(zz, turn):
        return pl.ds(pl.multiple_of(shard_at(zz, c) + part * turn, part), part)

    def z_piece(arr, zz, k):
        s = lax.rem(k, ZW)
        return weights[arr].at[place(zz, jnp.where(s == 2, 2 + par, s) if paired else s)]

    def y_piece(arr, zz, turn):
        return weights[arr].at[place(zz, 2 + turn)]

    def wz_copy(arr, zz, side, k, dev):
        piece = z_piece(arr, zz, k)
        return rcopy(piece, piece, wz_s.at[arr, side, k], wz_r.at[arr, side, k], dev)

    def wy_copy(arr, zz, side, hop, turn):
        piece = y_piece(arr, zz, turn)
        return rcopy(piece, piece, wy_s.at[arr, side, hop], wy_r.at[arr, side, hop], twin)

    def wd_copy(arr, zz, side, k):
        piece = z_piece(arr, zz, k)
        return rcopy(piece, piece, wd_s.at[arr, side, k], wd_r.at[arr, side, k], sib)

    def yd_copy(arr, zz, side, hop):
        piece = y_piece(arr, zz, 1 - par)
        return rcopy(piece, piece, yd_s.at[arr, side, hop], yd_r.at[arr, side, hop], sib)

    def own_copy(arr):
        piece = weights[arr].at[pl.ds(shard_at(z, c), shard)]
        return rcopy(piece, piece, wo_s.at[arr], wo_r.at[arr], sib)

    def w_first(arr):
        own_copy(arr).start()
        for k in range(ZW):
            wz_copy(arr, z, 0, jnp.int32(k), zdev(z + 1)).start()
            wz_copy(arr, z, 1, jnp.int32(k), zdev(z - 1)).start()

    def y_serve(arr, hop):
        hop = jnp.int32(hop)

        @pl.when(hop < HALF)
        def _():
            for side in range(2):
                wy_copy(arr, z, side, hop, 1 - par).wait_recv()
                yd_copy(arr, zside(side, hop), side, hop).start()

        @pl.when(hop == HALF)
        def _():
            wy_copy(arr, z, 0, hop, 1 - par).wait_recv()
            yd_copy(arr, at(z + HALF), 0, hop).start()

    def w_serve(arr, k):
        k = jnp.int32(k)
        hop = k // ZW + 1
        last_way = lax.rem(k, ZW) == 2

        @pl.when(hop < HALF)
        def _():
            for side in range(2):
                wz_copy(arr, z, side, k, zdev(z + 1)).wait_recv()

        @pl.when(hop < HALF - 1)
        def _():
            wz_copy(arr, at(z - hop), 0, k + ZW, zdev(z + 1)).start()
            wz_copy(arr, at(z + hop), 1, k + ZW, zdev(z - 1)).start()

        @pl.when(hop == HALF - 1)
        def _():
            wz_copy(arr, at(z - hop * sgn), 0, k + ZW, zdev(z + sgn)).start()

        @pl.when(hop < HALF)
        def _():
            for side in range(2):
                wd_copy(arr, zside(side, hop), side, k).start()
            if paired:
                @pl.when(last_way)
                def _():
                    for side in range(2):
                        wy_copy(arr, zside(side, hop), side, hop, par).start()

        @pl.when(hop == HALF)
        def _():
            wz_copy(arr, z, 0, k, zdev(z + 1)).wait_recv()
            wd_copy(arr, at(z + HALF), 0, k).start()
            if paired:
                pl.when(last_way)(lambda: wy_copy(arr, at(z + HALF), 0, hop, par).start())

        if arr == 0:
            pl.when(k == NP - ZW - 1)(lambda: w_first(1))
        if paired:
            pl.when((lax.rem(k, ZW) == 0) & (hop > 2))(lambda: y_serve(arr, hop - 2))

    served = [0]
    y_done = [0, 0]

    def count_y(arr, count):
        y_done[arr] = max(y_done[arr], (count - 1) // ZW - 1)

    def need_y(arr, hop):
        while paired and y_done[arr] < hop:
            y_done[arr] += 1
            y_serve(arr, y_done[arr])

    def serve(count):
        for _ in range(count):
            if served[0] == 2 * NP:
                return
            arr, k = served[0] // NP, served[0] % NP
            w_serve(arr, k)
            count_y(arr, k + 1)
            served[0] += 1
            if arr == 1 and k in (0, 2):
                need_y(0, HALF - 1 if k == 0 else HALF)

    lz_copy(z, 0, 1, zdev(z + 1)).start()
    lz_copy(z, 1, 1, zdev(z - 1)).start()
    ld_copy(z, 0, 0).start()
    for load in (loads[0], loads[1], loads[3]):
        load.wait()
    x_first(0)
    w_first(0)

    query_norm = normalize(ql[...], q_gain)
    scale = (PLAIN + ROTARY) ** (-0.5) * math.log2(math.e)
    queries = jnp.transpose(jnp.dot(query_norm, wq[...], preferred_element_type=f32) * scale)
    wide = PLAIN + ROTARY
    for h in range(HP):
        base = h * wide
        first = queries[base + PLAIN:base + PLAIN + half]
        second = queries[base + PLAIN + half:base + wide]
        qx[x, c, base:base + PLAIN, :] = queries[base:base + PLAIN].astype(bf)
        qx[x, c, base + PLAIN:base + PLAIN + half, :] = (first * cosine - second * sine).astype(bf)
        qx[x, c, base + PLAIN + half:base + wide, :] = (second * cosine + first * sine).astype(bf)
    x_first(1)
    q2t[...] = jnp.zeros_like(q2t)
    m_sc[...] = jnp.full_like(m_sc, -1e30)
    l_sc[...] = jnp.zeros_like(l_sc)
    o_sc[...] = jnp.zeros_like(o_sc)

    lz_step(1)
    loads[4].wait()
    x_relay(0)
    serve(1)
    if HALF > 2:
        lz_step(2)
        serve(1)
    x_relay(1)
    x_share(0)
    if HALF > 3:
        lz_step(3)
        serve(1)
    x_share(1)
    loads[2].wait()
    x_first(2)
    x_end(0)
    step = PLAIN + VALUE
    key_rows = []
    for jj in range(X // 2):
        by_row = jnp.transpose(WKV[c * (X // 2) + jj].astype(f32))
        for h in range(HP):
            key_rows.append(by_row[h * step:h * step + PLAIN])
            wvt[(jj * HP + h) * VALUE:(jj * HP + h + 1) * VALUE, :] = by_row[h * step + PLAIN:(h + 1) * step].astype(bf)
    wk[...] = jnp.transpose(jnp.concatenate(key_rows, axis=0)).astype(bf)
    if HALF > 4:
        lz_step(4)
        serve(2)
    x_end(1)
    for jj in range(X // 2):
        for h in range(HP):
            hc = jj * HP + h
            p, hh = hc // 2, hc % 2
            for cc in range(2):
                lanes = slice((2 * hh + cc) * T, (2 * hh + cc + 1) * T)
                q2t[p, hh * PLAIN:(hh + 1) * PLAIN, lanes] = qx[c * (X // 2) + jj, cc, h * wide:h * wide + PLAIN, :]
                q2t[p, LANES:LANES + ROTARY, lanes] = qx[c * (X // 2) + jj, cc, h * wide + PLAIN:(h + 1) * wide, :]
    begun = 4 if HALF > 4 else HALF - 1 if HALF > 2 else 1

    def attend(za, zb):
        lhs = jnp.concatenate(
            [
                jnp.concatenate(
                    [xb[zz, :, kb * share:(kb + 1) * share, :].reshape(2 * share, LANES) for zz in (za, zb)], axis=0
                )
                for kb in range(KB)
            ],
            axis=1,
        )
        rope = []
        for zz in (za, zb):
            for core in range(2):
                packed = xb[zz, core, KB * share:, :].astype(f32)
                for g in range(gsub):
                    rope.append(packed if g == 0 else pltpu.roll(packed, LANES - g * ROTARY, 1))
        rope = jnp.concatenate(rope, axis=0).astype(bf)
        kk = jnp.dot(lhs, wk[...], preferred_element_type=f32).astype(bf)
        vt = nt_dot(wvt[...], lhs).astype(bf)
        for p in range(HC // 2):
            k2 = jnp.concatenate([kk[:, p * LANES:(p + 1) * LANES], rope], axis=1)
            s_buf[p] = jnp.dot(k2, q2t[p], preferred_element_type=f32)
            old = m_sc[p:p + 1, :]
            new = jnp.maximum(old, jnp.max(s_buf[p], axis=0, keepdims=True))
            factor = jnp.exp2(old - new)
            m_sc[p:p + 1, :] = new
            expo = jnp.exp2(s_buf[p] - new)
            l_sc[p:p + 1, :] = l_sc[p:p + 1, :] * factor + jnp.sum(expo, axis=0, keepdims=True)
            weights_t = expo.astype(bf)
            for hh in range(2):
                h = 2 * p + hh
                lanes = slice(hh * 2 * T, (hh + 1) * 2 * T)
                o_sc[h] = o_sc[h] * factor[:, lanes] + jnp.dot(
                    vt[h * VALUE:(h + 1) * VALUE, :], weights_t[:, lanes], preferred_element_type=f32
                )

    base = served[0]
    rounds = HALF // 2

    def phase(u, carry):
        for s in range(2):
            t = 2 * u + 1 + s
            pl.when(t + begun <= HALF)(lambda: lz_step(t + begun))
            for n in range(2):
                k = base + 2 * (t - 1) + n
                pl.when(k < NP)(lambda: w_serve(0, k))
            if s == 0:
                pl.when(u == min(1, rounds - 1))(lambda: x_relay(2))
            else:
                pl.when(u == min(2, rounds - 1))(lambda: x_share(2))

            @pl.when(t < HALF)
            def _():
                for side in range(2):
                    ld_copy(z, side, t).wait_recv()

            @pl.when(t == HALF)
            def _():
                ld_copy(z, 0, t).wait_recv()
                ld_copy(z, 0, 0).wait_recv()

            attend(at(z - lax.rem(t, HALF)), at(z + t))
        return carry

    lax.fori_loop(0, rounds, phase, 0)
    served[0] = min(base + 2 * HALF, NP)
    count_y(0, served[0])

    heads = []
    for h in range(HC):
        p, hh = h // 2, h % 2
        heads.append(o_sc[h] / l_sc[p:p + 1, hh * 2 * T:(hh + 1) * 2 * T])
    lse[x] = jnp.zeros_like(lse[x])
    lse[x, 0:HC // 2, :] = m_sc[...] + jnp.log2(l_sc[...])
    level = [
        rcopy(lse.at[x], lse.at[x], ml_s.at[d - 1], ml_r.at[d - 1], xdev(d)) for d in range(1, X)
    ]
    for copy in level:
        copy.start()
    ours = jnp.transpose(jnp.concatenate(heads, axis=0)).astype(bf)
    for q in range(X):
        for cc in range(2):
            obuf[q, cc] = ours[cc * T + q * share:cc * T + (q + 1) * share]
    far = [rcopy(obuf.at[xat(2), i], relay.at[i], mh_s.at[i], mh_r.at[i], xdev(d)) for i, d in enumerate((1, -1))]
    near = [rcopy(obuf.at[xat(d)], orx.at[x], mo_s.at[i], mo_r.at[i], xdev(d)) for i, d in enumerate((1, -1))]
    for copy in far + near:
        copy.start()
    serve(2)
    passed = []
    for i, d in enumerate((1, -1)):
        far[i].wait_recv()
        passed.append(rcopy(relay.at[i], orx.at[xat(-d), i], mr_s.at[i], mr_r.at[i], xdev(d)))
        passed[-1].start()
    for copy in level:
        copy.wait_recv()
    top = jnp.maximum(jnp.maximum(lse[0], lse[1]), jnp.maximum(lse[2], lse[3]))
    shares = [jnp.exp2(lse[q] - top) for q in range(X)]
    norm = 1.0 / (shares[0] + shares[1] + shares[2] + shares[3])
    wts[...] = jnp.transpose(jnp.concatenate([part_of * norm for part_of in shares], axis=0))
    x_end(2)
    serve(1)
    for copy in near + passed:
        copy.wait_recv()

    def merged(cc):
        total = 0.0
        for q in range(X):
            coef = []
            for h in range(HC):
                p, hh = h // 2, h % 2
                column = wts[pl.ds(pl.multiple_of((2 * hh + cc) * T + x * share, share), share), :]
                coef.append(jnp.broadcast_to(column[:, q * 8 + p:q * 8 + p + 1], (share, VALUE)))
            source = orx[q, cc].astype(f32)
            total = total + jnp.concatenate(coef, axis=1) * source
        return total.astype(bf)

    orx[x] = obuf[x]
    width = HC * VALUE
    columns = pl.ds(pl.multiple_of(c * width, width), width)
    msend[...] = merged(1 - c)
    across = rcopy(msend, mixed.at[:, columns], md_s.at[0], md_r.at[0], sib)
    across.start()
    mixed[:, columns] = merged(c)
    serve(1)
    across.wait_recv()
    NB = 256
    for n in range(W // NB):
        cols = slice(n * NB, (n + 1) * NB)
        branch = 0.0
        for q in range(X):
            rows = HP * VALUE
            branch = branch + jnp.dot(
                mixed[:, q * rows:(q + 1) * rows], WO[q, :, cols], preferred_element_type=f32
            )
        mid[:, cols] = (hrow[:, cols].astype(f32) + branch).astype(bf)
    nb[rowsof(x), :] = normalize(mid[...], gain)
    def quarter_rows(q, i):
        return nb.at[pl.ds(pl.multiple_of(q * share + i * (share // 2), share // 2), share // 2)]

    def spread_copy(n, i, d):
        piece = quarter_rows(x, i if n == 0 else 1 - i)
        return rcopy(piece, piece, ag_s.at[n, i], ag_r.at[n, i], xdev(d))

    spread = [[spread_copy(n, i, d) for i, d in enumerate((1, -1))] for n in range(2)]
    for copy in spread[0] + spread[1]:
        copy.start()
    serve(3)
    onward = []
    for i, d in enumerate((1, -1)):
        spread[0][i].wait_recv()
        piece = quarter_rows(xat(-d), i)
        onward.append(rcopy(piece, piece, ah_s.at[i], ah_r.at[i], xdev(d)))
        onward[-1].start()
    serve(3)
    for copy in spread[1] + onward:
        copy.wait_recv()

    def wd_wait(arr, hop):
        for side in range(2 if hop < HALF else 1):
            for k in range(ZW * (hop - 1), ZW * hop):
                wd_copy(arr, z, side, jnp.int32(k)).wait_recv()
            if paired:
                yd_copy(arr, z, side, jnp.int32(hop)).wait_recv()

    while served[0] < NP:
        serve(1)
    need_y(0, HALF)
    own_copy(0).wait_recv()
    for hop in range(1, HALF + 1):
        wd_wait(0, hop)
    CUTS = 4
    per = F // NB // CUTS
    for stage in range(CUTS):
        def up(n, carry):
            cols = pl.ds(pl.multiple_of(n * NB, NB), NB)
            high = jnp.maximum(jnp.dot(nb[...], U[:, cols], preferred_element_type=f32), 0.0)
            act[:, cols] = (high * high).astype(bf)
            return carry
        lax.fori_loop(stage * per, (stage + 1) * per, up, 0)
        serve(2)

    def fa_copy(t, i, d):
        return rcopy(osend.at[t, xat(2), i], opart.at[t, i], fa_s.at[t, i], fa_r.at[t, i], xdev(d))

    def fo_copy(t, i, d):
        return rcopy(osend.at[t, xat(d)], orecv.at[t, i], fo_s.at[t, i], fo_r.at[t, i], xdev(d))

    direct = rcopy(osend.at[HALF - 1, xat(2)], ofar, fz_s.at[0], fz_r.at[0], xdev(2))

    def pair_of(t):
        return at(z - (t % HALF)), at(z + t)

    def pass_on(t):
        for i, d in enumerate((1, -1)):
            fa_copy(t, i, d).wait_recv()
            osend[t, xat(d), i] = (osend[t, xat(d), i].astype(f32) + opart[t, i].astype(f32)).astype(bf)
            fo_copy(t, i, d).start()

    for t in range(1, HALF + 1):
        while served[0] < min(NP + ZW * (t + 1) + 1, 2 * NP):
            serve(1)
        need_y(1, t)
        if t == HALF:
            own_copy(1).wait_recv()
        wd_wait(1, t)
        rhs = jnp.concatenate(
            [D[pl.ds(pl.multiple_of(zz * 2 * shard, 2 * shard), 2 * shard), :] for zz in pair_of(t)], axis=0
        )
        block = nt_dot(act[...], rhs).astype(bf)
        for q in range(X):
            for side in range(2):
                osend[t - 1, q, side] = block[q * share:(q + 1) * share, side * LANES:(side + 1) * LANES]
        if t < HALF:
            for i, d in enumerate((1, -1)):
                fa_copy(t - 1, i, d).start()
        else:
            direct.start()
            for i, d in enumerate((1, -1)):
                fo_copy(t - 1, i, d).start()
        if t > 1:
            pass_on(t - 2)
    for t in range(1, HALF + 1):
        for i, d in enumerate((1, -1)):
            fo_copy(t - 1, i, d).wait_recv()
        if t == HALF:
            direct.wait_recv()
        for side, zz in enumerate(pair_of(t)):
            cols = pl.ds(pl.multiple_of(zz * LANES, LANES), LANES)
            total = osend[t - 1, x, side].astype(f32)
            for i in range(2):
                total = total + orecv[t - 1, i, side].astype(f32)
            if t == HALF:
                total = total + ofar[side].astype(f32)
            out[:, cols] = (mid[:, cols].astype(f32) + total).astype(bf)

    for copy in level + far + near + passed + [across] + spread[0] + spread[1] + onward + [ld_copy(z, 0, 0), own_copy(0), own_copy(1)]:
        copy.wait_send()
    for t in range(HALF):
        for i, d in enumerate((1, -1)):
            if t < HALF - 1:
                fa_copy(t, i, d).wait_send()
            fo_copy(t, i, d).wait_send()
    direct.wait_send()
    for what in range(3):
        for i, d in enumerate((1, -1)):
            x1_copy(what, i, d).wait_send()
            x2_copy(what, i, d).wait_send()
        for n in range(X - 1 if what == 2 else X // 2):
            if what == 0:
                pl.when((1 - c) * (X // 2) + n != x)(lambda: xd_copy(0, n).wait_send())
            else:
                xd_copy(what, n).wait_send()

    def drain(t, carry):
        def one(side):
            lz_copy(z, side, t, zdev(z + 1)).wait_send()
            ld_copy(z, side, t).wait_send()
            for arr in range(2):
                for s in range(ZW):
                    wz_copy(arr, z, side, ZW * (t - 1) + s, zdev(z + 1)).wait_send()
                    wd_copy(arr, z, side, ZW * (t - 1) + s).wait_send()
                if paired:
                    wy_copy(arr, z, side, t, par).wait_send()
                    yd_copy(arr, z, side, t).wait_send()
        one(0)
        pl.when(t < HALF)(lambda: one(1))
        return carry
    lax.fori_loop(1, HALF + 1, drain, 0)


def fused_layer(Z, X, paired, kvl, key_t, up_own, dn_own, hid, ql, wq, wkv, wo, cos_t, sin_t, q_gain, kv_gain, gain):
    HALF = Z // 2
    T, W = hid.shape
    F = up_own.shape[1]
    share = T // X
    rows = kvl.shape[1] // LANES * share + share * ROTARY // LANES
    bf, f32 = jnp.bfloat16, jnp.float32
    DMA = pltpu.SemaphoreType.DMA
    any_ = pl.BlockSpec(memory_space=pl.ANY)
    vm = pl.BlockSpec(memory_space=pltpu.VMEM)
    R = kvl.shape[1]
    hc = wkv.shape[1] // (PLAIN + VALUE) * X // 2
    scratch = [
        pltpu.VMEM((Z, 2, rows, LANES), bf),
        pltpu.VMEM((T, LANES), f32),
        pltpu.VMEM((W, F), bf),
        pltpu.VMEM((W, F), bf),
        pltpu.VMEM((share, W), bf),
        pltpu.VMEM((X,) + wkv.shape, bf),
        pltpu.VMEM((X,) + wo.shape, bf),
        pltpu.VMEM((X, 2, wq.shape[1], T), bf),
        pltpu.VMEM((hc // 2, 2 * LANES, 4 * T), bf),
        pltpu.VMEM((R, hc * PLAIN), bf),
        pltpu.VMEM((hc * VALUE, R), bf),
        pltpu.VMEM((hc // 2, 4 * share, 4 * T), f32),
        pltpu.VMEM((hc // 2, 4 * T), f32),
        pltpu.VMEM((hc // 2, 4 * T), f32),
        pltpu.VMEM((hc, VALUE, 2 * T), f32),
        pltpu.VMEM((X, 2, share, hc * VALUE), bf),
        pltpu.VMEM((X, 2, share, hc * VALUE), bf),
        pltpu.VMEM((2, share, hc * VALUE), bf),
        pltpu.VMEM((X, 8, 4 * T), f32),
        pltpu.VMEM((4 * T, X * 8), f32),
        pltpu.VMEM((share, hc * VALUE), bf),
        pltpu.VMEM((share, 2 * hc * VALUE), bf),
        pltpu.VMEM((share, W), bf),
        pltpu.VMEM((T, W), bf),
        pltpu.VMEM((T, F), bf),
        pltpu.VMEM((HALF, X, 2, share, LANES), bf),
        pltpu.VMEM((HALF, 2, 2, share, LANES), bf),
        pltpu.VMEM((HALF, 2, share, LANES), bf),
        pltpu.VMEM((2, share, LANES), bf),
        DMA((5,)),
    ]
    for shape in (
        (2, HALF + 1), (2, HALF + 1),
        (2, 2, 4 * HALF), (2, 2, HALF + 1), (2, 2, 4 * HALF), (2, 2, HALF + 1), (2,),
        (3, 2), (3, 2), (3, X - 1), (X - 1,), (2,), (2,), (2,), (1,),
        (2, 2), (2,), (HALF, 2), (HALF, 2), (1,),
    ):
        scratch += [DMA(shape), DMA(shape)]
    return pl.pallas_call(
        functools.partial(layer_kernel, Z, X, paired),
        out_shape=jax.ShapeDtypeStruct((share, W), bf),
        in_specs=[vm, vm, any_, any_, any_, vm, vm, any_, any_] + [vm] * 5,
        out_specs=vm,
        scratch_shapes=scratch,
        compiler_params=pltpu.CompilerParams(
            collective_id=0, has_side_effects=True, vmem_limit_bytes=62 * 1024 * 1024
        ),
        name="layer",
    )(kvl, key_t, up_own, dn_own, hid, ql, wq, wkv, wo, cos_t, sin_t, q_gain, kv_gain, gain)


def on_device(
    hidden_in, query_latent_rows, key_value_latent, rotary_key, query_norm_gain, key_value_gain,
    query_up_weight, key_value_up_weight, out_proj, feed_gain, feed_up, feed_down,
):
    X = lax.axis_size("tp")
    Z = lax.axis_size("sp") // 2
    paired = lax.axis_size("grp") % 2 == 0
    T = hidden_in.shape[0]
    half = ROTARY // 2
    position = (lax.axis_index("sp") * T + jnp.arange(T)).astype(jnp.float32)
    inverse = 10000.0 ** (-jnp.arange(half, dtype=jnp.float32) * 2.0 / ROTARY)
    angles = inverse[:, None] * position[None, :]
    return fused_layer(
        Z, X, paired, key_value_latent, rotary_key.T, feed_up, feed_down.T, hidden_in, query_latent_rows,
        query_up_weight, key_value_up_weight, out_proj, jnp.cos(angles), jnp.sin(angles),
        query_norm_gain.reshape(-1, LANES), key_value_gain.reshape(-1, LANES), feed_gain.reshape(-1, LANES),
    )


def solution(mesh):
    return jax.shard_map(
        on_device,
        mesh=mesh,
        in_specs=(
            P(("grp", "sp"), None),
            P(("grp", "sp"), None),
            P(("grp", "sp"), None),
            P(("grp", "sp"), None),
            P(),
            P(),
            P(None, "tp"),
            P(None, "tp"),
            P("tp", None),
            P(),
            P("sp", "tp"),
            P("tp", "sp"),
        ),
        out_specs=P(("grp", "sp", "tp"), None),
        check_vma=False,
    )
```

```python
import functools
import math

import jax
import jax.numpy as jnp
from jax import lax
from jax.experimental import pallas as pl
from jax.experimental.pallas import tpu as pltpu
from jax.sharding import PartitionSpec as P

PLAIN = 64
ROTARY = 32
VALUE = 64
MESH = pl.DeviceIdType.MESH
LANES = 128


def normalize(values, gain_ref):
    floats = values.astype(jnp.float32)
    inverse = lax.rsqrt(jnp.mean(floats * floats, axis=-1, keepdims=True) + 1e-06)
    return jnp.concatenate(
        [
            floats[:, k * LANES:(k + 1) * LANES] * inverse * gain_ref[k:k + 1, :]
            for k in range(values.shape[1] // LANES)
        ],
        axis=1,
    ).astype(jnp.bfloat16)


def nt_dot(a, b):
    return lax.dot_general(a, b, (((1,), (1,)), ((), ())), preferred_element_type=jnp.float32)


def layer_kernel(
    Z, X, paired,
    kvl, key_t, up_own, dn_own, hid, ql, wq, wkv, wo, cos_t, sin_t, q_gain, kv_gain, gain,
    out,
    xb, turned_key, U, D, hrow, WKV, WO, qx, q2t, wk, wvt, s_buf, m_sc, l_sc, o_sc, obuf, orx, relay, lse, lrx, wts, mixed,
    mid, nb, act, osend, orecv, opart, ofar,
    loc_s, lz_s, lz_r, ld_s, ld_r, w_s, wz_r, wy_r, wd_r,
    x1_s, x1_r, x2_s, x2_r, xd_s, xd_r, ml_s, ml_r, mo_s, mo_r, mh_s, mh_r,
    ag_s, ag_r, ah_s, ah_r, fa_s, fa_r, fo_s, fo_r, fz_s, fz_r,
):
    HALF = Z // 2
    sp = lax.axis_index("sp")
    x = lax.axis_index("tp")
    z = sp // 2
    c = sp % 2
    sgn = 1 - 2 * c
    group = lax.axis_index("grp")
    par = group % 2
    T, W = nb.shape
    F = U.shape[1]
    share = T // X
    shard = up_own.shape[0]
    KB = kvl.shape[1] // LANES
    gsub = LANES // ROTARY
    grow = share // gsub
    HP = wkv.shape[1] // (PLAIN + VALUE)
    HC = HP * X // 2
    bf = jnp.bfloat16
    f32 = jnp.float32

    def at(zz):
        return lax.rem(zz + 2 * Z, Z)

    def zdev(zz):
        return {"sp": 2 * at(zz) + c}

    sib = {"sp": 2 * z + 1 - c}
    twin = {"grp": group + 1 - 2 * par}

    def xat(d):
        return lax.rem(x + d + X, X)

    def xdev(d):
        return {"tp": xat(d)}

    def rcopy(src, dst, ss, rs, dev):
        return pltpu.make_async_remote_copy(
            src_ref=src, dst_ref=dst, send_sem=ss, recv_sem=rs, device_id=dev, device_id_type=MESH
        )

    def zside(side, t):
        return at(z - t) if side == 0 else at(z + t)

    def shard_at(zz, core):
        return pl.multiple_of(zz * (2 * shard) + core * shard, shard)

    def rowsof(q):
        return pl.ds(pl.multiple_of(q * share, share), share)

    loads = [
        pltpu.make_async_copy(wkv, WKV.at[x], loc_s.at[0]),
        pltpu.make_async_copy(up_own, U.at[pl.ds(shard_at(z, c), shard)], loc_s.at[1]),
        pltpu.make_async_copy(wo, WO.at[x], loc_s.at[2]),
        pltpu.make_async_copy(hid.at[rowsof(x)], hrow, loc_s.at[3]),
        pltpu.make_async_copy(dn_own, D.at[pl.ds(shard_at(z, c), shard)], loc_s.at[4]),
    ]
    for load in loads:
        load.start()
    barrier = pltpu.get_barrier_semaphore()
    peers = [zdev(z + 1), zdev(z - 1), sib] + ([twin] if paired else [])
    peers += [{"sp": 2 * z + core, "tp": xat(d)} for d in range(1, X) for core in range(2)]
    for dev in peers:
        pl.semaphore_signal(barrier, inc=1, device_id=dev, device_id_type=MESH)

    latent = normalize(kvl[rowsof(x), :], kv_gain)
    for kb in range(KB):
        xb[z, c, kb * share:(kb + 1) * share, :] = latent[:, kb * LANES:(kb + 1) * LANES]
    cosine, sine = cos_t[...], sin_t[...]
    half = ROTARY // 2
    key_first = key_t[0:half, :].astype(f32)
    key_second = key_t[half:ROTARY, :].astype(f32)
    turned_key[...] = jnp.transpose(
        jnp.concatenate(
            [
                key_first * cosine - key_second * sine,
                key_second * cosine + key_first * sine,
                jnp.zeros((LANES - ROTARY, T), f32),
            ],
            axis=0,
        )
    )
    packed_key = 0.0
    for g in range(gsub):
        piece = turned_key[pl.ds(pl.multiple_of(x * share + g * grow, grow), grow), :]
        packed_key = packed_key + (piece if g == 0 else pltpu.roll(piece, g * ROTARY, 1))
    xb[z, c, KB * share:, :] = packed_key.astype(bf)
    pl.semaphore_wait(barrier, len(peers))

    def lz_copy(zz, hop, dev):
        piece = xb.at[zz, c]
        return rcopy(piece, piece, lz_s.at[0], lz_r.at[hop], dev)

    def ld_copy(zz, t):
        return rcopy(xb.at[zz, c], xb.at[zz, c], ld_s.at[0], ld_r.at[t], sib)

    def lz_wait(hop, count):
        pieces = xb.at[pl.ds(0, count), 0]
        rcopy(pieces, pieces, lz_s.at[0], lz_r.at[hop], sib).wait_recv()

    def ld_wait(t):
        rcopy(xb.at[0], xb.at[0], ld_s.at[0], ld_r.at[t], sib).wait_recv()

    def lz_step(i):
        i = jnp.int32(i)

        @pl.when(i < HALF)
        def _():
            lz_wait(i, 2)

        @pl.when(i < HALF - 1)
        def _():
            lz_copy(at(z - i), i + 1, zdev(z + 1)).start()
            lz_copy(at(z + i), i + 1, zdev(z - 1)).start()

        @pl.when(i == HALF - 1)
        def _():
            lz_copy(at(z - i * sgn), i + 1, zdev(z + sgn)).start()

        @pl.when(i < HALF)
        def _():
            for side in range(2):
                ld_copy(zside(side, i), i).start()

        @pl.when(i == HALF)
        def _():
            lz_wait(i, 1)
            ld_copy(at(z + HALF), i).start()

    kv_half, q_half, o_half = WKV.shape[1] // 2, qx.shape[2], WO.shape[1] // 2

    def x_piece(what, q, lo=0, parts=1):
        if what == 0:
            n = kv_half // parts
            return WKV.at[q, pl.ds(pl.multiple_of(c * kv_half + lo * n, n), n)]
        if what == 1:
            n = q_half // parts
            return qx.at[q, c, pl.ds(lo * n, n)]
        n = o_half // parts
        return WO.at[q, pl.ds(pl.multiple_of(c * o_half + lo * n, n), n)]

    def x1_copy(what, i, d):
        piece = x_piece(what, x)
        return rcopy(piece, piece, x1_s.at[what, i], x1_r.at[what, i], xdev(d))

    def x2_copy(what, i, d):
        piece = x_piece(what, xat(-d), i, 2)
        return rcopy(piece, piece, x2_s.at[what, i], x2_r.at[what, i], xdev(d))

    def xd_copy(what, n):
        if what == 2:
            piece = x_piece(2, xat(n + 1))
        else:
            piece = x_piece(what, (1 - c) * (X // 2) + n)
        return rcopy(piece, piece, xd_s.at[what, n], xd_r.at[what, n], sib)

    def x_first(what):
        for i, d in enumerate((1, -1)):
            x1_copy(what, i, d).start()

    def x_relay(what):
        for i, d in enumerate((1, -1)):
            x1_copy(what, i, d).wait_recv()
            x2_copy(what, i, d).start()

    def x_share(what):
        for i, d in enumerate((1, -1)):
            x2_copy(what, i, d).wait_recv()
        for n in range(X - 1 if what == 2 else X // 2):
            if what == 0:
                pl.when((1 - c) * (X // 2) + n != x)(lambda: xd_copy(0, n).start())
            else:
                xd_copy(what, n).start()

    def x_end(what):
        for n in range(X - 1 if what == 2 else X // 2):
            if what == 0:
                pl.when(c * (X // 2) + n != x)(lambda: xd_copy(0, n).wait_recv())
            else:
                xd_copy(what, n).wait_recv()

    weights = (U, D)
    ZW = 3 if paired else 4
    part = shard // 4
    NP = ZW * HALF

    def place(zz, turn):
        return pl.ds(pl.multiple_of(shard_at(zz, c) + part * turn, part), part)

    def z_piece(arr, zz, k):
        s = lax.rem(k, ZW)
        return weights[arr].at[place(zz, jnp.where(s == 2, 2 + par, s) if paired else s)]

    def y_piece(arr, zz, turn):
        return weights[arr].at[place(zz, 2 + turn)]

    def wz_copy(arr, zz, k, dev):
        piece = z_piece(arr, zz, k)
        return rcopy(piece, piece, w_s.at[0], wz_r.at[arr, k], dev)

    def wy_copy(arr, zz, hop, turn):
        piece = y_piece(arr, zz, turn)
        return rcopy(piece, piece, w_s.at[0], wy_r.at[arr, hop], twin)

    def to_sib(arr, piece, hop):
        return rcopy(piece, piece, w_s.at[1], wd_r.at[0 if arr == 0 else hop], sib)

    def w_rows(count):
        return weights[0].at[pl.ds(0, count)]

    def wz_wait(arr, k, count):
        rcopy(w_rows(count * part), w_rows(count * part), w_s.at[0], wz_r.at[arr, k], sib).wait_recv()

    def wy_wait(arr, hop, count):
        rcopy(w_rows(count * part), w_rows(count * part), w_s.at[0], wy_r.at[arr, hop], sib).wait_recv()

    def w_first(arr):
        to_sib(arr, weights[arr].at[pl.ds(shard_at(z, c), shard)], HALF).start()
        for k in range(ZW):
            wz_copy(arr, z, jnp.int32(k), zdev(z + 1)).start()
            wz_copy(arr, z, jnp.int32(k), zdev(z - 1)).start()

    def y_serve(arr, hop):
        hop = jnp.int32(hop)

        @pl.when(hop < HALF)
        def _():
            wy_wait(arr, hop, 2)
            for side in range(2):
                to_sib(arr, y_piece(arr, zside(side, hop), 1 - par), hop).start()

        @pl.when(hop == HALF)
        def _():
            wy_wait(arr, hop, 1)
            to_sib(arr, y_piece(arr, at(z + HALF), 1 - par), hop).start()

    def w_serve(arr, k):
        k = jnp.int32(k)
        hop = k // ZW + 1
        last_way = lax.rem(k, ZW) == 2

        @pl.when(hop < HALF)
        def _():
            wz_wait(arr, k, 2)

        @pl.when(hop < HALF - 1)
        def _():
            wz_copy(arr, at(z - hop), k + ZW, zdev(z + 1)).start()
            wz_copy(arr, at(z + hop), k + ZW, zdev(z - 1)).start()

        @pl.when(hop == HALF - 1)
        def _():
            wz_copy(arr, at(z - hop * sgn), k + ZW, zdev(z + sgn)).start()

        @pl.when(hop < HALF)
        def _():
            for side in range(2):
                to_sib(arr, z_piece(arr, zside(side, hop), k), hop).start()
            if paired:
                @pl.when(last_way)
                def _():
                    for side in range(2):
                        wy_copy(arr, zside(side, hop), hop, par).start()

        @pl.when(hop == HALF)
        def _():
            wz_wait(arr, k, 1)
            to_sib(arr, z_piece(arr, at(z + HALF), k), hop).start()
            if paired:
                pl.when(last_way)(lambda: wy_copy(arr, at(z + HALF), hop, par).start())

        if arr == 0:
            pl.when(k == NP - ZW - 1)(lambda: w_first(1))
        if paired:
            pl.when((lax.rem(k, ZW) == 0) & (hop > 2))(lambda: y_serve(arr, hop - 2))

    served = [0]
    y_done = [0, 0]

    def count_y(arr, count):
        y_done[arr] = max(y_done[arr], (count - 1) // ZW - 1)

    def need_y(arr, hop):
        while paired and y_done[arr] < hop:
            y_done[arr] += 1
            y_serve(arr, y_done[arr])

    def serve(count):
        for _ in range(count):
            if served[0] == 2 * NP:
                return
            arr, k = served[0] // NP, served[0] % NP
            w_serve(arr, k)
            count_y(arr, k + 1)
            served[0] += 1
            if arr == 1 and k in (0, 2):
                need_y(0, HALF - 1 if k == 0 else HALF)

    lz_copy(z, 1, zdev(z + 1)).start()
    lz_copy(z, 1, zdev(z - 1)).start()
    ld_copy(z, HALF).start()
    for load in (loads[0], loads[1], loads[3]):
        load.wait()
    x_first(0)
    w_first(0)

    query_norm = normalize(ql[...], q_gain)
    scale = (PLAIN + ROTARY) ** (-0.5) * math.log2(math.e)
    queries = jnp.transpose(jnp.dot(query_norm, wq[...], preferred_element_type=f32) * scale)
    wide = PLAIN + ROTARY
    for h in range(HP):
        base = h * wide
        first = queries[base + PLAIN:base + PLAIN + half]
        second = queries[base + PLAIN + half:base + wide]
        qx[x, c, base:base + PLAIN, :] = queries[base:base + PLAIN].astype(bf)
        qx[x, c, base + PLAIN:base + PLAIN + half, :] = (first * cosine - second * sine).astype(bf)
        qx[x, c, base + PLAIN + half:base + wide, :] = (second * cosine + first * sine).astype(bf)
    x_first(1)
    q2t[...] = jnp.zeros_like(q2t)
    m_sc[...] = jnp.full_like(m_sc, -1e30)
    l_sc[...] = jnp.zeros_like(l_sc)
    o_sc[...] = jnp.zeros_like(o_sc)

    lz_step(1)
    loads[4].wait()
    x_relay(0)
    serve(1)
    if HALF > 2:
        lz_step(2)
        serve(1)
    x_relay(1)
    x_share(0)
    if HALF > 3:
        lz_step(3)
        serve(1)
    x_share(1)
    loads[2].wait()
    x_first(2)
    x_end(0)
    step = PLAIN + VALUE
    key_rows = []
    for jj in range(X // 2):
        by_row = jnp.transpose(WKV[c * (X // 2) + jj].astype(f32))
        for h in range(HP):
            key_rows.append(by_row[h * step:h * step + PLAIN])
            wvt[(jj * HP + h) * VALUE:(jj * HP + h + 1) * VALUE, :] = by_row[h * step + PLAIN:(h + 1) * step].astype(bf)
    wk[...] = jnp.transpose(jnp.concatenate(key_rows, axis=0)).astype(bf)
    if HALF > 3:
        serve(2)
    x_end(1)
    for jj in range(X // 2):
        for h in range(HP):
            hc = jj * HP + h
            p, hh = hc // 2, hc % 2
            for cc in range(2):
                lanes = slice((2 * hh + cc) * T, (2 * hh + cc + 1) * T)
                q2t[p, hh * PLAIN:(hh + 1) * PLAIN, lanes] = qx[c * (X // 2) + jj, cc, h * wide:h * wide + PLAIN, :]
                q2t[p, LANES:LANES + ROTARY, lanes] = qx[c * (X // 2) + jj, cc, h * wide + PLAIN:(h + 1) * wide, :]
    begun = 3 if HALF > 3 else HALF - 1 if HALF > 2 else 1

    def attend(za, zb):
        lhs = jnp.concatenate(
            [
                jnp.concatenate(
                    [xb[zz, :, kb * share:(kb + 1) * share, :].reshape(2 * share, LANES) for zz in (za, zb)], axis=0
                )
                for kb in range(KB)
            ],
            axis=1,
        )
        rope = []
        for zz in (za, zb):
            for core in range(2):
                packed = xb[zz, core, KB * share:, :].astype(f32)
                for g in range(gsub):
                    rope.append(packed if g == 0 else pltpu.roll(packed, LANES - g * ROTARY, 1))
        rope = jnp.concatenate(rope, axis=0).astype(bf)
        kk = jnp.dot(lhs, wk[...], preferred_element_type=f32).astype(bf)
        vt = nt_dot(wvt[...], lhs).astype(bf)
        for p in range(HC // 2):
            k2 = jnp.concatenate([kk[:, p * LANES:(p + 1) * LANES], rope], axis=1)
            s_buf[p] = jnp.dot(k2, q2t[p], preferred_element_type=f32)
            old = m_sc[p:p + 1, :]
            new = jnp.maximum(old, jnp.max(s_buf[p], axis=0, keepdims=True))
            factor = jnp.exp2(old - new)
            m_sc[p:p + 1, :] = new
            expo = jnp.exp2(s_buf[p] - new)
            l_sc[p:p + 1, :] = l_sc[p:p + 1, :] * factor + jnp.sum(expo, axis=0, keepdims=True)
            weights_t = expo.astype(bf)
            for hh in range(2):
                h = 2 * p + hh
                lanes = slice(hh * 2 * T, (hh + 1) * 2 * T)
                o_sc[h] = o_sc[h] * factor[:, lanes] + jnp.dot(
                    vt[h * VALUE:(h + 1) * VALUE, :], weights_t[:, lanes], preferred_element_type=f32
                )

    base = served[0]
    rounds = HALF // 2

    def phase(u, carry):
        for s in range(2):
            t = 2 * u + 1 + s
            pl.when(t + begun <= HALF)(lambda: lz_step(t + begun))
            for n in range(2):
                k = base + 2 * (t - 1) + n
                pl.when(k < NP)(lambda: w_serve(0, k))
            if s == 0:
                pl.when(u == min(1, rounds - 1))(lambda: x_relay(2))
            else:
                pl.when(u == min(2, rounds - 1))(lambda: x_share(2))

            ld_wait(t)
            attend(at(z - lax.rem(t, HALF)), at(z + t))
        return carry

    lax.fori_loop(0, rounds, phase, 0)
    served[0] = min(base + 2 * HALF, NP)
    count_y(0, served[0])

    heads = []
    for h in range(HC):
        p, hh = h // 2, h % 2
        heads.append(o_sc[h] / l_sc[p:p + 1, hh * 2 * T:(hh + 1) * 2 * T])
    final = m_sc[...] + jnp.log2(l_sc[...])
    for cc in range(2):
        lse[cc] = jnp.concatenate(
            [
                final[h // 2:h // 2 + 1, (2 * (h % 2) + cc) * T:(2 * (h % 2) + cc + 1) * T]
                for h in range(HC)
            ],
            axis=0,
        )
    here = 2 * x + c

    def owner(d, core):
        return {"sp": 2 * z + core, "tp": xat(d)}

    level = [
        rcopy(lse.at[cc], lrx.at[here], ml_s.at[0], ml_r.at[0], owner(d, cc)) for d in range(1, X) for cc in range(2)
    ]
    level.append(rcopy(lse.at[1 - c], lrx.at[here], ml_s.at[0], ml_r.at[0], sib))
    for copy in level:
        copy.start()
    lrx[here] = lse[c]
    ours = jnp.transpose(jnp.concatenate(heads, axis=0)).astype(bf)
    for q in range(X):
        for cc in range(2):
            obuf[q, cc] = ours[cc * T + q * share:cc * T + (q + 1) * share]
    far = [rcopy(obuf.at[xat(2), i], relay.at[i], mh_s.at[i], mh_r.at[i], xdev(d)) for i, d in enumerate((1, -1))]
    near = [
        rcopy(obuf.at[xat(d), cc], orx.at[here], mo_s.at[0], mo_r.at[0], owner(d, cc))
        for d in (1, -1) for cc in range(2)
    ]
    near.append(rcopy(obuf.at[x, 1 - c], orx.at[here], mo_s.at[0], mo_r.at[0], sib))
    for copy in far + near:
        copy.start()
    orx[here] = obuf[x, c]
    serve(3)
    for i, d in enumerate((1, -1)):
        far[i].wait_recv()
        rcopy(relay.at[i], orx.at[2 * xat(-d) + c], mo_s.at[0], mo_r.at[0], owner(d, i)).start()
    others = 2 * X - 1

    def seven(ref, ss, rs):
        return rcopy(ref.at[pl.ds(0, others)], ref.at[pl.ds(0, others)], ss.at[0], rs.at[0], sib)

    seven(lrx, ml_s, ml_r).wait_recv()
    coefs = []
    for core in range(2):
        levels = [lrx[2 * q + core] for q in range(X)]
        top = functools.reduce(jnp.maximum, levels)
        parts = [jnp.exp2(level_of - top) for level_of in levels]
        norm = 1.0 / functools.reduce(jnp.add, parts)
        coefs += [part_of * norm for part_of in parts]
    wts[...] = jnp.transpose(jnp.concatenate(coefs, axis=0))
    x_end(2)
    serve(3)
    seven(orx, mo_s, mo_r).wait_recv()
    columns = wts[rowsof(x), :]
    for core in range(2):
        total = 0.0
        for q in range(X):
            first = (core * X + q) * HC
            coef = jnp.concatenate(
                [jnp.broadcast_to(columns[:, first + h:first + h + 1], (share, VALUE)) for h in range(HC)], axis=1
            )
            total = total + coef * orx[2 * q + core].astype(f32)
        mixed[:, core * HC * VALUE:(core + 1) * HC * VALUE] = total.astype(bf)
    NB = 256
    for n in range(W // NB):
        cols = slice(n * NB, (n + 1) * NB)
        branch = 0.0
        for q in range(X):
            rows = HP * VALUE
            branch = branch + jnp.dot(
                mixed[:, q * rows:(q + 1) * rows], WO[q, :, cols], preferred_element_type=f32
            )
        mid[:, cols] = (hrow[:, cols].astype(f32) + branch).astype(bf)
    nb[rowsof(x), :] = normalize(mid[...], gain)
    def quarter_rows(q, i):
        return nb.at[pl.ds(pl.multiple_of(q * share + i * (share // 2), share // 2), share // 2)]

    def spread_copy(n, i, d):
        piece = quarter_rows(x, i if n == 0 else 1 - i)
        return rcopy(piece, piece, ag_s.at[n, i], ag_r.at[n, i], xdev(d))

    spread = [[spread_copy(n, i, d) for i, d in enumerate((1, -1))] for n in range(2)]
    for copy in spread[0] + spread[1]:
        copy.start()
    serve(4)
    onward = []
    for i, d in enumerate((1, -1)):
        spread[0][i].wait_recv()
        piece = quarter_rows(xat(-d), i)
        onward.append(rcopy(piece, piece, ah_s.at[i], ah_r.at[i], xdev(d)))
        onward[-1].start()
    serve(4)
    for copy in spread[1] + onward:
        copy.wait_recv()

    def wd_wait(arr, hop, count):
        rcopy(w_rows(count), w_rows(count), w_s.at[1], wd_r.at[0 if arr == 0 else hop], sib).wait_recv()

    while served[0] < NP:
        serve(1)
    need_y(0, HALF)
    wd_wait(0, 0, Z * shard)
    CUTS = 4
    per = F // NB // CUTS
    for stage in range(CUTS):
        def up(n, carry):
            cols = pl.ds(pl.multiple_of(n * NB, NB), NB)
            high = jnp.maximum(jnp.dot(nb[...], U[:, cols], preferred_element_type=f32), 0.0)
            act[:, cols] = (high * high).astype(bf)
            return carry
        lax.fori_loop(stage * per, (stage + 1) * per, up, 0)
        serve(1)

    def fa_copy(t, i, d):
        return rcopy(osend.at[t, xat(2), i], opart.at[t, i], fa_s.at[0], fa_r.at[t], xdev(d))

    def fo_copy(t, i, d):
        return rcopy(osend.at[t, xat(d)], orecv.at[t, i], fo_s.at[0], fo_r.at[0], xdev(d))

    direct = rcopy(osend.at[HALF - 1, xat(2)], ofar, fz_s.at[0], fz_r.at[0], xdev(2))

    def pair_of(t):
        return at(z - (t % HALF)), at(z + t)

    def pass_on(t):
        rcopy(opart.at[t], opart.at[t], fa_s.at[0], fa_r.at[t], sib).wait_recv()
        for i, d in enumerate((1, -1)):
            osend[t, xat(d), i] = (osend[t, xat(d), i].astype(f32) + opart[t, i].astype(f32)).astype(bf)
            fo_copy(t, i, d).start()

    for t in range(1, HALF + 1):
        while served[0] < min(NP + ZW * (t + 1) + 1, 2 * NP):
            serve(1)
        need_y(1, t)
        wd_wait(1, t, 2 * shard)
        rhs = jnp.concatenate(
            [D[pl.ds(pl.multiple_of(zz * 2 * shard, 2 * shard), 2 * shard), :] for zz in pair_of(t)], axis=0
        )
        block = nt_dot(act[...], rhs).astype(bf)
        for q in range(X):
            for side in range(2):
                osend[t - 1, q, side] = block[q * share:(q + 1) * share, side * LANES:(side + 1) * LANES]
        if t < HALF:
            for i, d in enumerate((1, -1)):
                fa_copy(t - 1, i, d).start()
        else:
            direct.start()
            for i, d in enumerate((1, -1)):
                fo_copy(t - 1, i, d).start()
        if t > 1:
            pass_on(t - 2)
    rcopy(orecv, orecv, fo_s.at[0], fo_r.at[0], sib).wait_recv()
    direct.wait_recv()
    for t in range(1, HALF + 1):
        for side, zz in enumerate(pair_of(t)):
            cols = pl.ds(pl.multiple_of(zz * LANES, LANES), LANES)
            total = osend[t - 1, x, side].astype(f32)
            for i in range(2):
                total = total + orecv[t - 1, i, side].astype(f32)
            if t == HALF:
                total = total + ofar[side].astype(f32)
            out[:, cols] = (mid[:, cols].astype(f32) + total).astype(bf)

    for copy in far + spread[0] + spread[1] + onward + [direct]:
        copy.wait_send()
    seven(lrx, ml_s, ml_r).wait_send()
    seven(orx, mo_s, mo_r).wait_send()
    sent = opart.at[pl.ds(0, HALF - 1)]
    rcopy(sent, sent, fa_s.at[0], fa_r.at[0], sib).wait_send()
    rcopy(orecv, orecv, fo_s.at[0], fo_r.at[0], sib).wait_send()
    for what in range(3):
        for i, d in enumerate((1, -1)):
            x1_copy(what, i, d).wait_send()
            x2_copy(what, i, d).wait_send()
        for n in range(X - 1 if what == 2 else X // 2):
            if what == 0:
                pl.when((1 - c) * (X // 2) + n != x)(lambda: xd_copy(0, n).wait_send())
            else:
                xd_copy(what, n).wait_send()
    sent = xb.at[pl.ds(0, Z - 1), 0]
    rcopy(sent, sent, lz_s.at[0], lz_r.at[0], sib).wait_send()
    sent = xb.at[pl.ds(0, HALF)]
    rcopy(sent, sent, ld_s.at[0], ld_r.at[0], sib).wait_send()
    sent = w_rows(2 * (Z - 1) * 4 * part)
    rcopy(sent, sent, w_s.at[0], wz_r.at[0, 0], sib).wait_send()
    sent = w_rows(2 * Z * shard)
    rcopy(sent, sent, w_s.at[1], wd_r.at[0], sib).wait_send()


def fused_layer(Z, X, paired, kvl, key_t, up_own, dn_own, hid, ql, wq, wkv, wo, cos_t, sin_t, q_gain, kv_gain, gain):
    HALF = Z // 2
    T, W = hid.shape
    F = up_own.shape[1]
    share = T // X
    rows = kvl.shape[1] // LANES * share + share * ROTARY // LANES
    bf, f32 = jnp.bfloat16, jnp.float32
    DMA = pltpu.SemaphoreType.DMA
    any_ = pl.BlockSpec(memory_space=pl.ANY)
    vm = pl.BlockSpec(memory_space=pltpu.VMEM)
    R = kvl.shape[1]
    hc = wkv.shape[1] // (PLAIN + VALUE) * X // 2
    scratch = [
        pltpu.VMEM((Z, 2, rows, LANES), bf),
        pltpu.VMEM((T, LANES), f32),
        pltpu.VMEM((W, F), bf),
        pltpu.VMEM((W, F), bf),
        pltpu.VMEM((share, W), bf),
        pltpu.VMEM((X,) + wkv.shape, bf),
        pltpu.VMEM((X,) + wo.shape, bf),
        pltpu.VMEM((X, 2, wq.shape[1], T), bf),
        pltpu.VMEM((hc // 2, 2 * LANES, 4 * T), bf),
        pltpu.VMEM((R, hc * PLAIN), bf),
        pltpu.VMEM((hc * VALUE, R), bf),
        pltpu.VMEM((hc // 2, 4 * share, 4 * T), f32),
        pltpu.VMEM((hc // 2, 4 * T), f32),
        pltpu.VMEM((hc // 2, 4 * T), f32),
        pltpu.VMEM((hc, VALUE, 2 * T), f32),
        pltpu.VMEM((X, 2, share, hc * VALUE), bf),
        pltpu.VMEM((X * 2, share, hc * VALUE), bf),
        pltpu.VMEM((2, share, hc * VALUE), bf),
        pltpu.VMEM((2, hc, T), f32),
        pltpu.VMEM((X * 2, hc, T), f32),
        pltpu.VMEM((T, X * 2 * hc), f32),
        pltpu.VMEM((share, 2 * hc * VALUE), bf),
        pltpu.VMEM((share, W), bf),
        pltpu.VMEM((T, W), bf),
        pltpu.VMEM((T, F), bf),
        pltpu.VMEM((HALF, X, 2, share, LANES), bf),
        pltpu.VMEM((HALF, 2, 2, share, LANES), bf),
        pltpu.VMEM((HALF, 2, share, LANES), bf),
        pltpu.VMEM((2, share, LANES), bf),
        DMA((5,)),
    ]
    for shape in (
        (1,), (HALF + 1,), (1,), (HALF + 1,),
        (2,), (2, 4 * HALF if not paired else 3 * HALF), (2, HALF + 1), (HALF + 1,),
        (3, 2), (3, 2), (3, 2), (3, 2), (3, X - 1), (3, X - 1), (1,), (1,), (1,), (1,), (2,), (2,),
        (2, 2), (2, 2), (2,), (2,), (1,), (HALF,), (1,), (1,), (1,), (1,),
    ):
        scratch.append(DMA(shape))
    return pl.pallas_call(
        functools.partial(layer_kernel, Z, X, paired),
        out_shape=jax.ShapeDtypeStruct((share, W), bf),
        in_specs=[vm, vm, any_, any_, any_, vm, vm, any_, any_] + [vm] * 5,
        out_specs=vm,
        scratch_shapes=scratch,
        compiler_params=pltpu.CompilerParams(
            collective_id=0, has_side_effects=True, vmem_limit_bytes=62 * 1024 * 1024
        ),
        name="layer",
    )(kvl, key_t, up_own, dn_own, hid, ql, wq, wkv, wo, cos_t, sin_t, q_gain, kv_gain, gain)


def on_device(
    hidden_in, query_latent_rows, key_value_latent, rotary_key, query_norm_gain, key_value_gain,
    query_up_weight, key_value_up_weight, out_proj, feed_gain, feed_up, feed_down,
):
    X = lax.axis_size("tp")
    Z = lax.axis_size("sp") // 2
    paired = lax.axis_size("grp") % 2 == 0
    T = hidden_in.shape[0]
    half = ROTARY // 2
    position = (lax.axis_index("sp") * T + jnp.arange(T)).astype(jnp.float32)
    inverse = 10000.0 ** (-jnp.arange(half, dtype=jnp.float32) * 2.0 / ROTARY)
    angles = inverse[:, None] * position[None, :]
    return fused_layer(
        Z, X, paired, key_value_latent, rotary_key.T, feed_up, feed_down.T, hidden_in, query_latent_rows,
        query_up_weight, key_value_up_weight, out_proj, jnp.cos(angles), jnp.sin(angles),
        query_norm_gain.reshape(-1, LANES), key_value_gain.reshape(-1, LANES), feed_gain.reshape(-1, LANES),
    )


def solution(mesh):
    return jax.shard_map(
        on_device,
        mesh=mesh,
        in_specs=(
            P(("grp", "sp"), None),
            P(("grp", "sp"), None),
            P(("grp", "sp"), None),
            P(("grp", "sp"), None),
            P(),
            P(),
            P(None, "tp"),
            P(None, "tp"),
            P("tp", None),
            P(),
            P("sp", "tp"),
            P("tp", "sp"),
        ),
        out_specs=P(("grp", "sp", "tp"), None),
        check_vma=False,
    )
```

```python
import functools
import math

import jax
import jax.numpy as jnp
from jax import lax
from jax.experimental import pallas as pl
from jax.experimental.pallas import tpu as pltpu
from jax.sharding import PartitionSpec as P

PLAIN = 64
ROTARY = 32
VALUE = 64
MESH = pl.DeviceIdType.MESH
LANES = 128


def normalize(values, gain_ref):
    floats = values.astype(jnp.float32)
    inverse = lax.rsqrt(jnp.mean(floats * floats, axis=-1, keepdims=True) + 1e-06)
    return jnp.concatenate(
        [
            floats[:, k * LANES:(k + 1) * LANES] * inverse * gain_ref[k:k + 1, :]
            for k in range(values.shape[1] // LANES)
        ],
        axis=1,
    ).astype(jnp.bfloat16)


def nt_dot(a, b):
    return lax.dot_general(a, b, (((1,), (1,)), ((), ())), preferred_element_type=jnp.float32)


def layer_kernel(
    Z, X, paired,
    kvl, key_t, up_own, dn_own, hid, ql, wq, wkv, wo, cos_t, sin_t, q_gain, kv_gain, gain,
    out,
    xb, turned_key, U, D, hrow, WKV, WO, qx, q2t, wk, wvt, s_buf, m_sc, l_sc, o_sc, obuf, orx, relay, lse, lrx, wts, mixed,
    mid, nb, act, osend, orecv, opart, ofar,
    loc_s, lz_s, lz_r, ld_s, ld_r, w_s, wz_r, wy_r, wd_r,
    x1_s, x1_r, x2_s, x2_r, xd_s, xd_r, ml_s, ml_r, mo_s, mo_r, mh_s, mh_r,
    ag_s, ag_r, ah_s, ah_r, fa_s, fa_r, fo_s, fo_r, fz_s, fz_r,
):
    HALF = Z // 2
    sp = lax.axis_index("sp")
    x = lax.axis_index("tp")
    z = sp // 2
    c = sp % 2
    sgn = 1 - 2 * c
    group = lax.axis_index("grp")
    par = group % 2
    T, W = nb.shape
    F = U.shape[1]
    share = T // X
    shard = up_own.shape[0]
    KB = kvl.shape[1] // LANES
    gsub = LANES // ROTARY
    grow = share // gsub
    HP = wkv.shape[1] // (PLAIN + VALUE)
    HC = HP * X // 2
    bf = jnp.bfloat16
    f32 = jnp.float32

    def at(zz):
        return lax.rem(zz + 2 * Z, Z)

    def zdev(zz):
        return {"sp": 2 * at(zz) + c}

    sib = {"sp": 2 * z + 1 - c}
    twin = {"grp": group + 1 - 2 * par}

    def xat(d):
        return lax.rem(x + d + X, X)

    def xdev(d):
        return {"tp": xat(d)}

    def rcopy(src, dst, ss, rs, dev):
        return pltpu.make_async_remote_copy(
            src_ref=src, dst_ref=dst, send_sem=ss, recv_sem=rs, device_id=dev, device_id_type=MESH
        )

    def zside(side, t):
        return at(z - t) if side == 0 else at(z + t)

    def shard_at(zz, core):
        return pl.multiple_of(zz * (2 * shard) + core * shard, shard)

    def rowsof(q):
        return pl.ds(pl.multiple_of(q * share, share), share)

    loads = [
        pltpu.make_async_copy(wkv, WKV.at[x], loc_s.at[0]),
        pltpu.make_async_copy(up_own, U.at[pl.ds(shard_at(z, c), shard)], loc_s.at[1]),
        pltpu.make_async_copy(wo, WO.at[x], loc_s.at[2]),
        pltpu.make_async_copy(hid.at[rowsof(x)], hrow, loc_s.at[3]),
        pltpu.make_async_copy(dn_own, D.at[pl.ds(shard_at(z, c), shard)], loc_s.at[4]),
    ]
    for load in loads:
        load.start()
    barrier = pltpu.get_barrier_semaphore()
    peers = [zdev(z + 1), zdev(z - 1), sib] + ([twin] if paired else [])
    peers += [{"sp": 2 * z + core, "tp": xat(d)} for d in range(1, X) for core in range(2)]
    for dev in peers:
        pl.semaphore_signal(barrier, inc=1, device_id=dev, device_id_type=MESH)

    latent = normalize(kvl[rowsof(x), :], kv_gain)
    for kb in range(KB):
        xb[z, c, kb * share:(kb + 1) * share, :] = latent[:, kb * LANES:(kb + 1) * LANES]
    cosine, sine = cos_t[...], sin_t[...]
    half = ROTARY // 2
    key_first = key_t[0:half, :].astype(f32)
    key_second = key_t[half:ROTARY, :].astype(f32)
    turned_key[...] = jnp.transpose(
        jnp.concatenate(
            [
                key_first * cosine - key_second * sine,
                key_second * cosine + key_first * sine,
                jnp.zeros((LANES - ROTARY, T), f32),
            ],
            axis=0,
        )
    )
    packed_key = 0.0
    for g in range(gsub):
        piece = turned_key[pl.ds(pl.multiple_of(x * share + g * grow, grow), grow), :]
        packed_key = packed_key + (piece if g == 0 else pltpu.roll(piece, g * ROTARY, 1))
    xb[z, c, KB * share:, :] = packed_key.astype(bf)
    pl.semaphore_wait(barrier, len(peers))

    cuts = (KB * share // 2, KB * share // 2 + grow)

    def lz_copy(zz, hop, dev, n):
        piece = xb.at[zz, c, pl.ds(n * cuts[0], cuts[n])]
        return rcopy(piece, piece, lz_s.at[0], lz_r.at[n, hop], dev)

    def ld_copy(zz, t):
        return rcopy(xb.at[zz, c], xb.at[zz, c], ld_s.at[0], ld_r.at[t], sib)

    def lz_wait(hop, count, n):
        pieces = xb.at[pl.ds(0, count), 0, pl.ds(n * cuts[0], cuts[n])]
        rcopy(pieces, pieces, lz_s.at[0], lz_r.at[n, hop], sib).wait_recv()

    def ld_wait(t):
        rcopy(xb.at[0], xb.at[0], ld_s.at[0], ld_r.at[t], sib).wait_recv()

    def lz_step(i):
        i = jnp.int32(i)
        for n in range(2):
            pl.when(i < HALF)(lambda: lz_wait(i, 2, n))

            @pl.when(i < HALF - 1)
            def _():
                lz_copy(at(z - i), i + 1, zdev(z + 1), n).start()
                lz_copy(at(z + i), i + 1, zdev(z - 1), n).start()

            @pl.when(i == HALF - 1)
            def _():
                lz_copy(at(z - i * sgn), i + 1, zdev(z + sgn), n).start()

            pl.when(i == HALF)(lambda: lz_wait(i, 1, n))

        @pl.when(i < HALF)
        def _():
            for side in range(2):
                ld_copy(zside(side, i), i).start()

        @pl.when(i == HALF)
        def _():
            ld_copy(at(z + HALF), i).start()

    kv_half, q_half, o_half = WKV.shape[1] // 2, qx.shape[2], WO.shape[1] // 2

    def x_piece(what, q, lo=0, parts=1):
        if what == 0:
            n = kv_half // parts
            return WKV.at[q, pl.ds(pl.multiple_of(c * kv_half + lo * n, n), n)]
        if what == 1:
            n = q_half // parts
            return qx.at[q, c, pl.ds(lo * n, n)]
        n = o_half // parts
        return WO.at[q, pl.ds(pl.multiple_of(c * o_half + lo * n, n), n)]

    def x1_copy(what, i, d):
        piece = x_piece(what, x)
        return rcopy(piece, piece, x1_s.at[what, i], x1_r.at[what, i], xdev(d))

    def x2_copy(what, i, d):
        piece = x_piece(what, xat(-d), i, 2)
        return rcopy(piece, piece, x2_s.at[what, i], x2_r.at[what, i], xdev(d))

    def xd_copy(what, n):
        if what == 2:
            piece = x_piece(2, xat(n + 1))
        else:
            piece = x_piece(what, (1 - c) * (X // 2) + n)
        return rcopy(piece, piece, xd_s.at[what, n], xd_r.at[what, n], sib)

    def x_first(what):
        for i, d in enumerate((1, -1)):
            x1_copy(what, i, d).start()

    def x_relay(what):
        for i, d in enumerate((1, -1)):
            x1_copy(what, i, d).wait_recv()
            x2_copy(what, i, d).start()

    def x_share(what):
        for i, d in enumerate((1, -1)):
            x2_copy(what, i, d).wait_recv()
        for n in range(X - 1 if what == 2 else X // 2):
            if what == 0:
                pl.when((1 - c) * (X // 2) + n != x)(lambda: xd_copy(0, n).start())
            else:
                xd_copy(what, n).start()

    def x_end(what):
        for n in range(X - 1 if what == 2 else X // 2):
            if what == 0:
                pl.when(c * (X // 2) + n != x)(lambda: xd_copy(0, n).wait_recv())
            else:
                xd_copy(what, n).wait_recv()

    weights = (U, D)
    ZW = (2, 3) if paired else (4, 4)
    part = shard // 4
    NP = tuple(ways * HALF for ways in ZW)

    def place(zz, turn, count=1):
        return pl.ds(pl.multiple_of(shard_at(zz, c) + part * turn, part), part * count)

    def z_piece(arr, zz, k):
        s = lax.rem(k, ZW[arr])
        if paired:
            s = 2 * par + s if arr == 0 else jnp.where(s == 2, 2 + par, s)
        return weights[arr].at[place(zz, s)]

    def y_piece(arr, zz, turn):
        return weights[arr].at[place(zz, 2 * turn, 2) if arr == 0 else place(zz, 2 + turn)]

    def wz_copy(arr, zz, k, dev):
        piece = z_piece(arr, zz, k)
        return rcopy(piece, piece, w_s.at[0], wz_r.at[arr, k], dev)

    def wy_copy(arr, zz, hop, turn):
        piece = y_piece(arr, zz, turn)
        return rcopy(piece, piece, w_s.at[0], wy_r.at[arr, hop], twin)

    def to_sib(arr, piece, hop):
        return rcopy(piece, piece, w_s.at[1], wd_r.at[0 if arr == 0 else hop], sib)

    def w_rows(count):
        return weights[0].at[pl.ds(0, count)]

    def wz_wait(arr, k, count):
        rcopy(w_rows(count * part), w_rows(count * part), w_s.at[0], wz_r.at[arr, k], sib).wait_recv()

    def wy_wait(arr, hop, count):
        count = count * (4 - ZW[arr])
        rcopy(w_rows(count * part), w_rows(count * part), w_s.at[0], wy_r.at[arr, hop], sib).wait_recv()

    def w_first(arr):
        to_sib(arr, weights[arr].at[pl.ds(shard_at(z, c), shard)], HALF).start()
        for k in range(ZW[arr]):
            wz_copy(arr, z, jnp.int32(k), zdev(z + 1)).start()
            wz_copy(arr, z, jnp.int32(k), zdev(z - 1)).start()

    def y_serve(arr, hop):
        hop = jnp.int32(hop)

        @pl.when(hop < HALF)
        def _():
            wy_wait(arr, hop, 2)
            for side in range(2):
                to_sib(arr, y_piece(arr, zside(side, hop), 1 - par), hop).start()

        @pl.when(hop == HALF)
        def _():
            wy_wait(arr, hop, 1)
            to_sib(arr, y_piece(arr, at(z + HALF), 1 - par), hop).start()

    def w_serve(arr, k):
        k = jnp.int32(k)
        hop = k // ZW[arr] + 1
        last_way = lax.rem(k, ZW[arr]) == ZW[arr] - 1

        @pl.when(hop < HALF)
        def _():
            wz_wait(arr, k, 2)

        @pl.when(hop < HALF - 1)
        def _():
            wz_copy(arr, at(z - hop), k + ZW[arr], zdev(z + 1)).start()
            wz_copy(arr, at(z + hop), k + ZW[arr], zdev(z - 1)).start()

        @pl.when(hop == HALF - 1)
        def _():
            wz_copy(arr, at(z - hop * sgn), k + ZW[arr], zdev(z + sgn)).start()

        @pl.when(hop < HALF)
        def _():
            for side in range(2):
                to_sib(arr, z_piece(arr, zside(side, hop), k), hop).start()
            if paired:
                @pl.when(last_way)
                def _():
                    for side in range(2):
                        wy_copy(arr, zside(side, hop), hop, par).start()

        @pl.when(hop == HALF)
        def _():
            wz_wait(arr, k, 1)
            to_sib(arr, z_piece(arr, at(z + HALF), k), hop).start()
            if paired:
                pl.when(last_way)(lambda: wy_copy(arr, at(z + HALF), hop, par).start())

        if arr == 0:
            pl.when(k == ZW[0] * (AHEAD - 1))(lambda: w_first(1))

    served = [0]
    y_done = [0, 0]

    def need_y(arr, hop):
        while paired and y_done[arr] < hop:
            y_done[arr] += 1
            y_serve(arr, y_done[arr])

    AHEAD = min(4, HALF)
    order = []
    for hop in range(HALF):
        order += [(0, ZW[0] * hop + n) for n in range(ZW[0])]
        if hop >= AHEAD:
            order += [(1, ZW[1] * (hop - AHEAD) + n) for n in range(ZW[1])]
    order += [(1, k) for k in range(ZW[1] * (HALF - AHEAD), NP[1])]

    def serve(count):
        for _ in range(count):
            if served[0] == len(order):
                return
            arr, k = order[served[0]]
            w_serve(arr, k)
            served[0] += 1
            if arr == 1 and k % ZW[1] == 0:
                need_y(1, k // ZW[1] - 1)

    def serve_until(arr, hop):
        while served[0] <= order.index((arr, ZW[arr] * min(hop, HALF) - 1)):
            serve(1)

    for n in range(2):
        lz_copy(z, 1, zdev(z + 1), n).start()
        lz_copy(z, 1, zdev(z - 1), n).start()
    ld_copy(z, HALF).start()
    for load in (loads[0], loads[1], loads[3]):
        load.wait()
    x_first(0)
    w_first(0)

    query_norm = normalize(ql[...], q_gain)
    scale = (PLAIN + ROTARY) ** (-0.5) * math.log2(math.e)
    queries = jnp.transpose(jnp.dot(query_norm, wq[...], preferred_element_type=f32) * scale)
    wide = PLAIN + ROTARY
    for h in range(HP):
        base = h * wide
        first = queries[base + PLAIN:base + PLAIN + half]
        second = queries[base + PLAIN + half:base + wide]
        qx[x, c, base:base + PLAIN, :] = queries[base:base + PLAIN].astype(bf)
        qx[x, c, base + PLAIN:base + PLAIN + half, :] = (first * cosine - second * sine).astype(bf)
        qx[x, c, base + PLAIN + half:base + wide, :] = (second * cosine + first * sine).astype(bf)
    x_first(1)
    q2t[...] = jnp.zeros_like(q2t)
    m_sc[...] = jnp.full_like(m_sc, -1e30)
    l_sc[...] = jnp.zeros_like(l_sc)
    o_sc[...] = jnp.zeros_like(o_sc)

    begun = 0

    def lz_next():
        nonlocal begun
        if begun < min(5, HALF - 1):
            begun += 1
            lz_step(begun)
            serve(1)

    loads[4].wait()
    lz_next()
    x_relay(0)
    lz_next()
    x_relay(1)
    lz_next()
    x_share(0)
    lz_next()
    x_share(1)
    loads[2].wait()
    x_first(2)
    x_end(0)
    step = PLAIN + VALUE
    key_rows = []
    for jj in range(X // 2):
        by_row = jnp.transpose(WKV[c * (X // 2) + jj].astype(f32))
        for h in range(HP):
            key_rows.append(by_row[h * step:h * step + PLAIN])
            wvt[(jj * HP + h) * VALUE:(jj * HP + h + 1) * VALUE, :] = by_row[h * step + PLAIN:(h + 1) * step].astype(bf)
    wk[...] = jnp.transpose(jnp.concatenate(key_rows, axis=0)).astype(bf)
    lz_next()
    x_end(1)
    for jj in range(X // 2):
        for h in range(HP):
            hc = jj * HP + h
            p, hh = hc // 2, hc % 2
            for cc in range(2):
                lanes = slice((2 * hh + cc) * T, (2 * hh + cc + 1) * T)
                q2t[p, hh * PLAIN:(hh + 1) * PLAIN, lanes] = qx[c * (X // 2) + jj, cc, h * wide:h * wide + PLAIN, :]
                q2t[p, LANES:LANES + ROTARY, lanes] = qx[c * (X // 2) + jj, cc, h * wide + PLAIN:(h + 1) * wide, :]

    def attend(za, zb):
        lhs = jnp.concatenate(
            [
                jnp.concatenate(
                    [xb[zz, :, kb * share:(kb + 1) * share, :].reshape(2 * share, LANES) for zz in (za, zb)], axis=0
                )
                for kb in range(KB)
            ],
            axis=1,
        )
        rope = []
        for zz in (za, zb):
            for core in range(2):
                packed = xb[zz, core, KB * share:, :].astype(f32)
                for g in range(gsub):
                    rope.append(packed if g == 0 else pltpu.roll(packed, LANES - g * ROTARY, 1))
        rope = jnp.concatenate(rope, axis=0).astype(bf)
        kk = jnp.dot(lhs, wk[...], preferred_element_type=f32).astype(bf)
        vt = nt_dot(wvt[...], lhs).astype(bf)
        def scores(p):
            k2 = jnp.concatenate([kk[:, p * LANES:(p + 1) * LANES], rope], axis=1)
            s_buf[p] = jnp.dot(k2, q2t[p], preferred_element_type=f32)

        scores(0)
        for p in range(HC // 2):
            if p + 1 < HC // 2:
                scores(p + 1)
            old = m_sc[p:p + 1, :]
            new = jnp.maximum(old, jnp.max(s_buf[p], axis=0, keepdims=True))
            factor = jnp.exp2(old - new)
            m_sc[p:p + 1, :] = new
            expo = jnp.exp2(s_buf[p] - new)
            l_sc[p:p + 1, :] = l_sc[p:p + 1, :] * factor + jnp.sum(expo, axis=0, keepdims=True)
            weights_t = expo.astype(bf)
            for hh in range(2):
                h = 2 * p + hh
                lanes = slice(hh * 2 * T, (hh + 1) * 2 * T)
                o_sc[h] = o_sc[h] * factor[:, lanes] + jnp.dot(
                    vt[h * VALUE:(h + 1) * VALUE, :], weights_t[:, lanes], preferred_element_type=f32
                )

    base = served[0]
    rounds = HALF // 2
    turn = ZW[0] * min(AHEAD + 1, HALF)

    def phase(u, carry):
        for s in range(2):
            t = 2 * u + 1 + s
            pl.when(t + begun <= HALF)(lambda: lz_step(t + begun))
            k = base + t - 1
            pl.when(k < turn)(lambda: w_serve(0, k))
            pl.when(k >= turn)(lambda: w_serve(1, jnp.maximum(k - turn, 0)))
            if paired and s == 1:
                y_serve(0, u + 1)
            if s == 0:
                pl.when(u == min(1, rounds - 1))(lambda: x_relay(2))
            else:
                pl.when(u == min(2, rounds - 1))(lambda: x_share(2))

            ld_wait(t)
            attend(at(z - lax.rem(t, HALF)), at(z + t))
        return carry

    lax.fori_loop(0, rounds, phase, 0)
    served[0] = base + HALF
    y_done[0] = rounds

    heads = []
    for h in range(HC):
        p, hh = h // 2, h % 2
        heads.append(o_sc[h] / l_sc[p:p + 1, hh * 2 * T:(hh + 1) * 2 * T])
    final = m_sc[...] + jnp.log2(l_sc[...])
    for cc in range(2):
        lse[cc] = jnp.concatenate(
            [
                final[h // 2:h // 2 + 1, (2 * (h % 2) + cc) * T:(2 * (h % 2) + cc + 1) * T]
                for h in range(HC)
            ],
            axis=0,
        )
    here = 2 * x + c

    def owner(d, core):
        return {"sp": 2 * z + core, "tp": xat(d)}

    level = [
        rcopy(lse.at[cc], lrx.at[here], ml_s.at[0], ml_r.at[0], owner(d, cc)) for d in range(1, X) for cc in range(2)
    ]
    level.append(rcopy(lse.at[1 - c], lrx.at[here], ml_s.at[0], ml_r.at[0], sib))
    for copy in level:
        copy.start()
    lrx[here] = lse[c]
    ours = jnp.transpose(jnp.concatenate(heads, axis=0)).astype(bf)
    for q in range(X):
        for cc in range(2):
            obuf[q, cc] = ours[cc * T + q * share:cc * T + (q + 1) * share]
    far = [rcopy(obuf.at[xat(2), i], relay.at[i], mh_s.at[i], mh_r.at[i], xdev(d)) for i, d in enumerate((1, -1))]
    near = [
        rcopy(obuf.at[xat(d), cc], orx.at[here], mo_s.at[0], mo_r.at[0], owner(d, cc))
        for d in (1, -1) for cc in range(2)
    ]
    near.append(rcopy(obuf.at[x, 1 - c], orx.at[here], mo_s.at[0], mo_r.at[0], sib))
    for copy in far + near:
        copy.start()
    orx[here] = obuf[x, c]
    serve(4)
    for i, d in enumerate((1, -1)):
        far[i].wait_recv()
        rcopy(relay.at[i], orx.at[2 * xat(-d) + c], mo_s.at[0], mo_r.at[0], owner(d, i)).start()
    others = 2 * X - 1

    def seven(ref, ss, rs):
        return rcopy(ref.at[pl.ds(0, others)], ref.at[pl.ds(0, others)], ss.at[0], rs.at[0], sib)

    seven(lrx, ml_s, ml_r).wait_recv()
    coefs = []
    for core in range(2):
        levels = [lrx[2 * q + core] for q in range(X)]
        top = functools.reduce(jnp.maximum, levels)
        parts = [jnp.exp2(level_of - top) for level_of in levels]
        norm = 1.0 / functools.reduce(jnp.add, parts)
        coefs += [part_of * norm for part_of in parts]
    wts[...] = jnp.transpose(jnp.concatenate(coefs, axis=0))
    x_end(2)
    serve(4)
    need_y(0, HALF - 3)
    seven(orx, mo_s, mo_r).wait_recv()
    columns = wts[rowsof(x), :]
    for core in range(2):
        total = 0.0
        for q in range(X):
            first = (core * X + q) * HC
            coef = jnp.concatenate(
                [jnp.broadcast_to(columns[:, first + h:first + h + 1], (share, VALUE)) for h in range(HC)], axis=1
            )
            total = total + coef * orx[2 * q + core].astype(f32)
        mixed[:, core * HC * VALUE:(core + 1) * HC * VALUE] = total.astype(bf)
    NB = 256
    for n in range(W // NB):
        cols = slice(n * NB, (n + 1) * NB)
        branch = 0.0
        for q in range(X):
            rows = HP * VALUE
            branch = branch + jnp.dot(
                mixed[:, q * rows:(q + 1) * rows], WO[q, :, cols], preferred_element_type=f32
            )
        mid[:, cols] = (hrow[:, cols].astype(f32) + branch).astype(bf)
    nb[rowsof(x), :] = normalize(mid[...], gain)
    def quarter_rows(q, i):
        return nb.at[pl.ds(pl.multiple_of(q * share + i * (share // 2), share // 2), share // 2)]

    def spread_copy(n, i, d):
        piece = quarter_rows(x, i if n == 0 else 1 - i)
        return rcopy(piece, piece, ag_s.at[n, i], ag_r.at[n, i], xdev(d))

    spread = [[spread_copy(n, i, d) for i, d in enumerate((1, -1))] for n in range(2)]
    for copy in spread[0] + spread[1]:
        copy.start()
    need_y(0, HALF - 2)
    serve(5)
    onward = []
    for i, d in enumerate((1, -1)):
        spread[0][i].wait_recv()
        piece = quarter_rows(xat(-d), i)
        onward.append(rcopy(piece, piece, ah_s.at[i], ah_r.at[i], xdev(d)))
        onward[-1].start()
    serve(4)
    need_y(0, HALF - 1)
    serve(1)
    for copy in spread[1] + onward:
        copy.wait_recv()

    def wd_wait(arr, hop, count):
        rcopy(w_rows(count), w_rows(count), w_s.at[1], wd_r.at[0 if arr == 0 else hop], sib).wait_recv()

    serve_until(0, HALF)
    need_y(0, HALF)
    wd_wait(0, 0, Z * shard)
    CUTS = 4
    per = F // NB // CUTS
    for stage in range(CUTS):
        def up(n, carry):
            cols = pl.ds(pl.multiple_of(n * NB, NB), NB)
            high = jnp.maximum(jnp.dot(nb[...], U[:, cols], preferred_element_type=f32), 0.0)
            act[:, cols] = (high * high).astype(bf)
            return carry
        lax.fori_loop(stage * per, (stage + 1) * per, up, 0)
        serve(2)

    def fa_copy(t, i, d):
        return rcopy(osend.at[t, xat(2), i], opart.at[t, i], fa_s.at[0], fa_r.at[t], xdev(d))

    def fo_copy(t, i, d):
        return rcopy(osend.at[t, xat(d)], orecv.at[t, i], fo_s.at[0], fo_r.at[0], xdev(d))

    LAG = 3
    direct = rcopy(osend.at[HALF - 1, xat(2)], ofar, fz_s.at[0], fz_r.at[0], xdev(2))

    def pair_of(t):
        return at(z - (t % HALF)), at(z + t)

    def pass_on(t):
        rcopy(opart.at[t], opart.at[t], fa_s.at[0], fa_r.at[t], sib).wait_recv()
        for i, d in enumerate((1, -1)):
            osend[t, xat(d), i] = (osend[t, xat(d), i].astype(f32) + opart[t, i].astype(f32)).astype(bf)
            fo_copy(t, i, d).start()

    for t in range(1, HALF + 1):
        serve_until(1, t + 1)
        need_y(1, t)
        wd_wait(1, t, 2 * shard)
        rhs = jnp.concatenate(
            [D[pl.ds(pl.multiple_of(zz * 2 * shard, 2 * shard), 2 * shard), :] for zz in pair_of(t)], axis=0
        )
        block = nt_dot(act[...], rhs).astype(bf)
        for q in range(X):
            for side in range(2):
                osend[t - 1, q, side] = block[q * share:(q + 1) * share, side * LANES:(side + 1) * LANES]
        if t < HALF:
            for i, d in enumerate((1, -1)):
                fa_copy(t - 1, i, d).start()
        else:
            direct.start()
            for i, d in enumerate((1, -1)):
                fo_copy(t - 1, i, d).start()
        if t > LAG:
            pass_on(t - 1 - LAG)
    for t in range(max(HALF - LAG, 0), HALF - 1):
        pass_on(t)
    rcopy(orecv, orecv, fo_s.at[0], fo_r.at[0], sib).wait_recv()
    direct.wait_recv()
    for t in range(1, HALF + 1):
        for side, zz in enumerate(pair_of(t)):
            cols = pl.ds(pl.multiple_of(zz * LANES, LANES), LANES)
            total = osend[t - 1, x, side].astype(f32)
            for i in range(2):
                total = total + orecv[t - 1, i, side].astype(f32)
            if t == HALF:
                total = total + ofar[side].astype(f32)
            out[:, cols] = (mid[:, cols].astype(f32) + total).astype(bf)

    for copy in far + spread[0] + spread[1] + onward + [direct]:
        copy.wait_send()
    seven(lrx, ml_s, ml_r).wait_send()
    seven(orx, mo_s, mo_r).wait_send()
    sent = opart.at[pl.ds(0, HALF - 1)]
    rcopy(sent, sent, fa_s.at[0], fa_r.at[0], sib).wait_send()
    rcopy(orecv, orecv, fo_s.at[0], fo_r.at[0], sib).wait_send()
    for what in range(3):
        for i, d in enumerate((1, -1)):
            x1_copy(what, i, d).wait_send()
            x2_copy(what, i, d).wait_send()
        for n in range(X - 1 if what == 2 else X // 2):
            if what == 0:
                pl.when((1 - c) * (X // 2) + n != x)(lambda: xd_copy(0, n).wait_send())
            else:
                xd_copy(what, n).wait_send()
    sent = xb.at[pl.ds(0, Z - 1), 0]
    rcopy(sent, sent, lz_s.at[0], lz_r.at[0, 0], sib).wait_send()
    sent = xb.at[pl.ds(0, HALF)]
    rcopy(sent, sent, ld_s.at[0], ld_r.at[0], sib).wait_send()
    sent = w_rows(2 * (Z - 1) * 4 * part)
    rcopy(sent, sent, w_s.at[0], wz_r.at[0, 0], sib).wait_send()
    sent = w_rows(2 * Z * shard)
    rcopy(sent, sent, w_s.at[1], wd_r.at[0], sib).wait_send()


def fused_layer(Z, X, paired, kvl, key_t, up_own, dn_own, hid, ql, wq, wkv, wo, cos_t, sin_t, q_gain, kv_gain, gain):
    HALF = Z // 2
    T, W = hid.shape
    F = up_own.shape[1]
    share = T // X
    rows = kvl.shape[1] // LANES * share + share * ROTARY // LANES
    bf, f32 = jnp.bfloat16, jnp.float32
    DMA = pltpu.SemaphoreType.DMA
    any_ = pl.BlockSpec(memory_space=pl.ANY)
    vm = pl.BlockSpec(memory_space=pltpu.VMEM)
    R = kvl.shape[1]
    hc = wkv.shape[1] // (PLAIN + VALUE) * X // 2
    scratch = [
        pltpu.VMEM((Z, 2, rows, LANES), bf),
        pltpu.VMEM((T, LANES), f32),
        pltpu.VMEM((W, F), bf),
        pltpu.VMEM((W, F), bf),
        pltpu.VMEM((share, W), bf),
        pltpu.VMEM((X,) + wkv.shape, bf),
        pltpu.VMEM((X,) + wo.shape, bf),
        pltpu.VMEM((X, 2, wq.shape[1], T), bf),
        pltpu.VMEM((hc // 2, 2 * LANES, 4 * T), bf),
        pltpu.VMEM((R, hc * PLAIN), bf),
        pltpu.VMEM((hc * VALUE, R), bf),
        pltpu.VMEM((hc // 2, 4 * share, 4 * T), f32),
        pltpu.VMEM((hc // 2, 4 * T), f32),
        pltpu.VMEM((hc // 2, 4 * T), f32),
        pltpu.VMEM((hc, VALUE, 2 * T), f32),
        pltpu.VMEM((X, 2, share, hc * VALUE), bf),
        pltpu.VMEM((X * 2, share, hc * VALUE), bf),
        pltpu.VMEM((2, share, hc * VALUE), bf),
        pltpu.VMEM((2, hc, T), f32),
        pltpu.VMEM((X * 2, hc, T), f32),
        pltpu.VMEM((T, X * 2 * hc), f32),
        pltpu.VMEM((share, 2 * hc * VALUE), bf),
        pltpu.VMEM((share, W), bf),
        pltpu.VMEM((T, W), bf),
        pltpu.VMEM((T, F), bf),
        pltpu.VMEM((HALF, X, 2, share, LANES), bf),
        pltpu.VMEM((HALF, 2, 2, share, LANES), bf),
        pltpu.VMEM((HALF, 2, share, LANES), bf),
        pltpu.VMEM((2, share, LANES), bf),
        DMA((5,)),
    ]
    for shape in (
        (1,), (2, HALF + 1), (1,), (HALF + 1,),
        (2,), (2, 4 * HALF), (2, HALF + 1), (HALF + 1,),
        (3, 2), (3, 2), (3, 2), (3, 2), (3, X - 1), (3, X - 1), (1,), (1,), (1,), (1,), (2,), (2,),
        (2, 2), (2, 2), (2,), (2,), (1,), (HALF,), (1,), (1,), (1,), (1,),
    ):
        scratch.append(DMA(shape))
    return pl.pallas_call(
        functools.partial(layer_kernel, Z, X, paired),
        out_shape=jax.ShapeDtypeStruct((share, W), bf),
        in_specs=[vm, vm, any_, any_, any_, vm, vm, any_, any_] + [vm] * 5,
        out_specs=vm,
        scratch_shapes=scratch,
        compiler_params=pltpu.CompilerParams(
            collective_id=0, has_side_effects=True, vmem_limit_bytes=62 * 1024 * 1024
        ),
        name="layer",
    )(kvl, key_t, up_own, dn_own, hid, ql, wq, wkv, wo, cos_t, sin_t, q_gain, kv_gain, gain)


def on_device(
    hidden_in, query_latent_rows, key_value_latent, rotary_key, query_norm_gain, key_value_gain,
    query_up_weight, key_value_up_weight, out_proj, feed_gain, feed_up, feed_down,
):
    X = lax.axis_size("tp")
    Z = lax.axis_size("sp") // 2
    paired = lax.axis_size("grp") % 2 == 0
    T = hidden_in.shape[0]
    half = ROTARY // 2
    position = (lax.axis_index("sp") * T + jnp.arange(T)).astype(jnp.float32)
    inverse = 10000.0 ** (-jnp.arange(half, dtype=jnp.float32) * 2.0 / ROTARY)
    angles = inverse[:, None] * position[None, :]
    return fused_layer(
        Z, X, paired, key_value_latent, rotary_key.T, feed_up, feed_down.T, hidden_in, query_latent_rows,
        query_up_weight, key_value_up_weight, out_proj, jnp.cos(angles), jnp.sin(angles),
        query_norm_gain.reshape(-1, LANES), key_value_gain.reshape(-1, LANES), feed_gain.reshape(-1, LANES),
    )


def solution(mesh):
    return jax.shard_map(
        on_device,
        mesh=mesh,
        in_specs=(
            P(("grp", "sp"), None),
            P(("grp", "sp"), None),
            P(("grp", "sp"), None),
            P(("grp", "sp"), None),
            P(),
            P(),
            P(None, "tp"),
            P(None, "tp"),
            P("tp", None),
            P(),
            P("sp", "tp"),
            P("tp", "sp"),
        ),
        out_specs=P(("grp", "sp", "tp"), None),
        check_vma=False,
    )
```

```python
import functools
import math

import jax
import jax.numpy as jnp
from jax import lax
from jax.experimental import pallas as pl
from jax.experimental.pallas import tpu as pltpu
from jax.sharding import PartitionSpec as P

PLAIN = 64
ROTARY = 32
VALUE = 64
MESH = pl.DeviceIdType.MESH
LANES = 128


def normalize(values, gain_ref):
    floats = values.astype(jnp.float32)
    inverse = lax.rsqrt(jnp.mean(floats * floats, axis=-1, keepdims=True) + 1e-06)
    return jnp.concatenate(
        [
            floats[:, k * LANES:(k + 1) * LANES] * inverse * gain_ref[k:k + 1, :]
            for k in range(values.shape[1] // LANES)
        ],
        axis=1,
    ).astype(jnp.bfloat16)


def nt_dot(a, b):
    return lax.dot_general(a, b, (((1,), (1,)), ((), ())), preferred_element_type=jnp.float32)


def layer_kernel(
    Z, X, paired,
    kvl, key_t, up_own, dn_own, hid, ql, wq, wkv, wo, cos_t, sin_t, q_gain, kv_gain, gain,
    out,
    xb, turned_key, U, D, hrow, WKV, WO, qx, q2t, wk, wvt, s_buf, m_sc, l_sc, o_sc, obuf, orx, relay, lse, lrx, wts, mixed,
    mid, nb, act, osend, orecv, opart, ofar,
    loc_s, lz_s, lz_r, ld_s, ld_r, w_s, wz_r, wy_r, wd_r,
    x1_s, x1_r, x2_s, x2_r, xd_s, xd_r, ml_s, ml_r, mo_s, mo_r, mh_s, mh_r,
    ag_s, ag_r, ah_s, ah_r, fa_s, fa_r, fo_s, fo_r, fz_s, fz_r,
):
    HALF = Z // 2
    sp = lax.axis_index("sp")
    x = lax.axis_index("tp")
    z = sp // 2
    c = sp % 2
    sgn = 1 - 2 * c
    group = lax.axis_index("grp")
    par = group % 2
    T, W = nb.shape
    F = U.shape[1]
    share = T // X
    shard = up_own.shape[0]
    KB = kvl.shape[1] // LANES
    gsub = LANES // ROTARY
    grow = share // gsub
    HP = wkv.shape[1] // (PLAIN + VALUE)
    HC = HP * X // 2
    bf = jnp.bfloat16
    f32 = jnp.float32

    def at(zz):
        return lax.rem(zz + 2 * Z, Z)

    def zdev(zz):
        return {"sp": 2 * at(zz) + c}

    sib = {"sp": 2 * z + 1 - c}
    twin = {"grp": group + 1 - 2 * par}

    def xat(d):
        return lax.rem(x + d + X, X)

    def xdev(d):
        return {"tp": xat(d)}

    def rcopy(src, dst, ss, rs, dev):
        return pltpu.make_async_remote_copy(
            src_ref=src, dst_ref=dst, send_sem=ss, recv_sem=rs, device_id=dev, device_id_type=MESH
        )

    def zside(side, t):
        return at(z - t) if side == 0 else at(z + t)

    def shard_at(zz, core):
        return pl.multiple_of(zz * (2 * shard) + core * shard, shard)

    def rowsof(q):
        return pl.ds(pl.multiple_of(q * share, share), share)

    loads = [
        pltpu.make_async_copy(wkv, WKV.at[x], loc_s.at[0]),
        pltpu.make_async_copy(up_own, U.at[pl.ds(shard_at(z, c), shard)], loc_s.at[1]),
        pltpu.make_async_copy(wo, WO.at[x], loc_s.at[2]),
        pltpu.make_async_copy(hid.at[rowsof(x)], hrow, loc_s.at[3]),
        pltpu.make_async_copy(dn_own, D.at[pl.ds(shard_at(z, c), shard)], loc_s.at[4]),
    ]
    for load in loads:
        load.start()
    barrier = pltpu.get_barrier_semaphore()
    peers = [zdev(z + 1), zdev(z - 1), sib] + ([twin] if paired else [])
    peers += [{"sp": 2 * z + core, "tp": xat(d)} for d in range(1, X) for core in range(2)]
    for dev in peers:
        pl.semaphore_signal(barrier, inc=1, device_id=dev, device_id_type=MESH)

    latent = normalize(kvl[rowsof(x), :], kv_gain)
    for kb in range(KB):
        xb[z, c, kb * share:(kb + 1) * share, :] = latent[:, kb * LANES:(kb + 1) * LANES]
    cosine, sine = cos_t[...], sin_t[...]
    half = ROTARY // 2
    key_first = key_t[0:half, :].astype(f32)
    key_second = key_t[half:ROTARY, :].astype(f32)
    turned_key[...] = jnp.transpose(
        jnp.concatenate(
            [
                key_first * cosine - key_second * sine,
                key_second * cosine + key_first * sine,
                jnp.zeros((LANES - ROTARY, T), f32),
            ],
            axis=0,
        )
    )
    packed_key = 0.0
    for g in range(gsub):
        piece = turned_key[pl.ds(pl.multiple_of(x * share + g * grow, grow), grow), :]
        packed_key = packed_key + (piece if g == 0 else pltpu.roll(piece, g * ROTARY, 1))
    xb[z, c, KB * share:, :] = packed_key.astype(bf)
    pl.semaphore_wait(barrier, len(peers))

    cuts = (KB * share // 2, KB * share // 2 + grow)

    def lz_copy(zz, hop, dev, n):
        piece = xb.at[zz, c, pl.ds(n * cuts[0], cuts[n])]
        return rcopy(piece, piece, lz_s.at[0], lz_r.at[n, hop], dev)

    def ld_copy(zz, t):
        return rcopy(xb.at[zz, c], xb.at[zz, c], ld_s.at[0], ld_r.at[t], sib)

    def lz_wait(hop, count, n):
        pieces = xb.at[pl.ds(0, count), 0, pl.ds(n * cuts[0], cuts[n])]
        rcopy(pieces, pieces, lz_s.at[0], lz_r.at[n, hop], sib).wait_recv()

    def ld_wait(t):
        rcopy(xb.at[0], xb.at[0], ld_s.at[0], ld_r.at[t], sib).wait_recv()

    def lz_step(i):
        i = jnp.int32(i)
        for n in range(2):
            pl.when(i < HALF)(lambda: lz_wait(i, 2, n))

            @pl.when(i < HALF - 1)
            def _():
                lz_copy(at(z - i), i + 1, zdev(z + 1), n).start()
                lz_copy(at(z + i), i + 1, zdev(z - 1), n).start()

            @pl.when(i == HALF - 1)
            def _():
                lz_copy(at(z - i * sgn), i + 1, zdev(z + sgn), n).start()

            pl.when(i == HALF)(lambda: lz_wait(i, 1, n))

        @pl.when(i < HALF)
        def _():
            for side in range(2):
                ld_copy(zside(side, i), i).start()

        @pl.when(i == HALF)
        def _():
            ld_copy(at(z + HALF), i).start()

    kv_half, q_half, o_half = WKV.shape[1] // 2, qx.shape[2], WO.shape[1] // 2

    def x_piece(what, q, lo=0, parts=1):
        if what == 0:
            n = kv_half // parts
            return WKV.at[q, pl.ds(pl.multiple_of(c * kv_half + lo * n, n), n)]
        if what == 1:
            n = q_half // parts
            return qx.at[q, c, pl.ds(lo * n, n)]
        n = o_half // parts
        return WO.at[q, pl.ds(pl.multiple_of(c * o_half + lo * n, n), n)]

    def x1_copy(what, i, d):
        piece = x_piece(what, x)
        return rcopy(piece, piece, x1_s.at[what, i], x1_r.at[what, i], xdev(d))

    def x2_copy(what, i, d):
        piece = x_piece(what, xat(-d), i, 2)
        return rcopy(piece, piece, x2_s.at[what, i], x2_r.at[what, i], xdev(d))

    def xd_copy(what, n):
        if what == 2:
            piece = x_piece(2, xat(n + 1))
        else:
            piece = x_piece(what, (1 - c) * (X // 2) + n)
        return rcopy(piece, piece, xd_s.at[what, n], xd_r.at[what, n], sib)

    def x_first(what):
        for i, d in enumerate((1, -1)):
            x1_copy(what, i, d).start()

    def x_relay(what):
        for i, d in enumerate((1, -1)):
            x1_copy(what, i, d).wait_recv()
            x2_copy(what, i, d).start()

    def x_share(what):
        for i, d in enumerate((1, -1)):
            x2_copy(what, i, d).wait_recv()
        for n in range(X - 1 if what == 2 else X // 2):
            if what == 0:
                pl.when((1 - c) * (X // 2) + n != x)(lambda: xd_copy(0, n).start())
            else:
                xd_copy(what, n).start()

    def x_end(what):
        for n in range(X - 1 if what == 2 else X // 2):
            if what == 0:
                pl.when(c * (X // 2) + n != x)(lambda: xd_copy(0, n).wait_recv())
            else:
                xd_copy(what, n).wait_recv()

    weights = (U, D)
    ZW = (2, 3) if paired else (4, 4)
    part = shard // 4
    NP = tuple(ways * HALF for ways in ZW)

    def place(zz, turn, count=1):
        return pl.ds(pl.multiple_of(shard_at(zz, c) + part * turn, part), part * count)

    def z_piece(arr, zz, k):
        s = lax.rem(k, ZW[arr])
        if paired:
            s = 2 * par + s if arr == 0 else jnp.where(s == 2, 2 + par, s)
        return weights[arr].at[place(zz, s)]

    def y_piece(arr, zz, turn):
        return weights[arr].at[place(zz, 2 * turn, 2) if arr == 0 else place(zz, 2 + turn)]

    def wz_copy(arr, zz, k, dev):
        piece = z_piece(arr, zz, k)
        return rcopy(piece, piece, w_s.at[0], wz_r.at[arr, k], dev)

    def wy_copy(arr, zz, hop, turn):
        piece = y_piece(arr, zz, turn)
        return rcopy(piece, piece, w_s.at[0], wy_r.at[arr, hop], twin)

    def to_sib(arr, piece, hop):
        return rcopy(piece, piece, w_s.at[1], wd_r.at[0 if arr == 0 else hop], sib)

    def w_rows(count):
        return weights[0].at[pl.ds(0, count)]

    def wz_wait(arr, k, count):
        rcopy(w_rows(count * part), w_rows(count * part), w_s.at[0], wz_r.at[arr, k], sib).wait_recv()

    def wy_wait(arr, hop, count):
        count = count * (4 - ZW[arr])
        rcopy(w_rows(count * part), w_rows(count * part), w_s.at[0], wy_r.at[arr, hop], sib).wait_recv()

    def w_first(arr):
        to_sib(arr, weights[arr].at[pl.ds(shard_at(z, c), shard)], HALF).start()
        for k in range(ZW[arr]):
            wz_copy(arr, z, jnp.int32(k), zdev(z + 1)).start()
            wz_copy(arr, z, jnp.int32(k), zdev(z - 1)).start()

    def y_serve(arr, hop):
        hop = jnp.int32(hop)

        @pl.when(hop < HALF)
        def _():
            wy_wait(arr, hop, 2)
            for side in range(2):
                to_sib(arr, y_piece(arr, zside(side, hop), 1 - par), hop).start()

        @pl.when(hop == HALF)
        def _():
            wy_wait(arr, hop, 1)
            to_sib(arr, y_piece(arr, at(z + HALF), 1 - par), hop).start()

    AHEAD = min(4, HALF)
    LATER = max(HALF - AHEAD - 1, 0)

    def y_send(arr, hop):
        for side in range(2):
            wy_copy(arr, zside(side, hop), hop, par).start()

    def w_serve(arr, k):
        k = jnp.int32(k)
        hop = k // ZW[arr] + 1
        last_way = lax.rem(k, ZW[arr]) == ZW[arr] - 1

        @pl.when(hop < HALF)
        def _():
            wz_wait(arr, k, 2)

        @pl.when(hop < HALF - 1)
        def _():
            wz_copy(arr, at(z - hop), k + ZW[arr], zdev(z + 1)).start()
            wz_copy(arr, at(z + hop), k + ZW[arr], zdev(z - 1)).start()

        @pl.when(hop == HALF - 1)
        def _():
            wz_copy(arr, at(z - hop * sgn), k + ZW[arr], zdev(z + sgn)).start()

        @pl.when(hop < HALF)
        def _():
            for side in range(2):
                to_sib(arr, z_piece(arr, zside(side, hop), k), hop).start()
            if paired:
                @pl.when(last_way & (hop > LATER) if arr == 1 else last_way)
                def _():
                    y_send(arr, hop)

        @pl.when(hop == HALF)
        def _():
            wz_wait(arr, k, 1)
            to_sib(arr, z_piece(arr, at(z + HALF), k), hop).start()
            if paired:
                pl.when(last_way)(lambda: wy_copy(arr, at(z + HALF), hop, par).start())

        if arr == 0:
            pl.when(k == ZW[0] * (AHEAD - 1))(lambda: w_first(1))

    served = [0]
    y_done = [0, 0]

    def need_y(arr, hop):
        while paired and y_done[arr] < hop:
            y_done[arr] += 1
            y_serve(arr, y_done[arr])

    order = []
    for hop in range(HALF):
        order += [(0, ZW[0] * hop + n) for n in range(ZW[0])]
        if hop >= AHEAD:
            order += [(1, ZW[1] * (hop - AHEAD) + n) for n in range(ZW[1])]
    order += [(1, k) for k in range(ZW[1] * (HALF - AHEAD), NP[1])]

    def serve(count):
        for _ in range(count):
            if served[0] == len(order):
                return
            arr, k = order[served[0]]
            w_serve(arr, k)
            served[0] += 1
            if (arr, k) == (0, NP[0] - 1) and paired:
                for hop in range(1, LATER + 1):
                    y_send(1, jnp.int32(hop))
            if arr == 1 and k % ZW[1] == 0:
                need_y(1, k // ZW[1] - 3)

    def serve_until(arr, hop):
        while served[0] <= order.index((arr, ZW[arr] * min(hop, HALF) - 1)):
            serve(1)

    for n in range(2):
        lz_copy(z, 1, zdev(z + 1), n).start()
        lz_copy(z, 1, zdev(z - 1), n).start()
    ld_copy(z, HALF).start()
    for load in (loads[0], loads[1], loads[3]):
        load.wait()
    x_first(0)
    w_first(0)

    query_norm = normalize(ql[...], q_gain)
    scale = (PLAIN + ROTARY) ** (-0.5) * math.log2(math.e)
    queries = jnp.transpose(jnp.dot(query_norm, wq[...], preferred_element_type=f32) * scale)
    wide = PLAIN + ROTARY
    for h in range(HP):
        base = h * wide
        first = queries[base + PLAIN:base + PLAIN + half]
        second = queries[base + PLAIN + half:base + wide]
        qx[x, c, base:base + PLAIN, :] = queries[base:base + PLAIN].astype(bf)
        qx[x, c, base + PLAIN:base + PLAIN + half, :] = (first * cosine - second * sine).astype(bf)
        qx[x, c, base + PLAIN + half:base + wide, :] = (second * cosine + first * sine).astype(bf)
    x_first(1)
    q2t[...] = jnp.zeros_like(q2t)
    m_sc[...] = jnp.full_like(m_sc, -1e30)
    l_sc[...] = jnp.zeros_like(l_sc)
    o_sc[...] = jnp.zeros_like(o_sc)

    begun = 0

    def lz_next():
        nonlocal begun
        if begun < min(5, HALF - 1):
            begun += 1
            lz_step(begun)
            serve(1)

    loads[4].wait()
    lz_next()
    x_relay(0)
    lz_next()
    x_relay(1)
    lz_next()
    x_share(0)
    lz_next()
    x_share(1)
    loads[2].wait()
    x_first(2)
    x_end(0)
    step = PLAIN + VALUE
    key_rows = []
    for jj in range(X // 2):
        by_row = jnp.transpose(WKV[c * (X // 2) + jj].astype(f32))
        for h in range(HP):
            key_rows.append(by_row[h * step:h * step + PLAIN])
            wvt[(jj * HP + h) * VALUE:(jj * HP + h + 1) * VALUE, :] = by_row[h * step + PLAIN:(h + 1) * step].astype(bf)
    wk[...] = jnp.transpose(jnp.concatenate(key_rows, axis=0)).astype(bf)
    lz_next()
    x_end(1)
    for jj in range(X // 2):
        for h in range(HP):
            hc = jj * HP + h
            p, hh = hc // 2, hc % 2
            for cc in range(2):
                lanes = slice((2 * hh + cc) * T, (2 * hh + cc + 1) * T)
                q2t[p, hh * PLAIN:(hh + 1) * PLAIN, lanes] = qx[c * (X // 2) + jj, cc, h * wide:h * wide + PLAIN, :]
                q2t[p, LANES:LANES + ROTARY, lanes] = qx[c * (X // 2) + jj, cc, h * wide + PLAIN:(h + 1) * wide, :]

    def attend(za, zb):
        lhs = jnp.concatenate(
            [
                jnp.concatenate(
                    [xb[zz, :, kb * share:(kb + 1) * share, :].reshape(2 * share, LANES) for zz in (za, zb)], axis=0
                )
                for kb in range(KB)
            ],
            axis=1,
        )
        rope = []
        for zz in (za, zb):
            for core in range(2):
                packed = xb[zz, core, KB * share:, :].astype(f32)
                for g in range(gsub):
                    rope.append(packed if g == 0 else pltpu.roll(packed, LANES - g * ROTARY, 1))
        rope = jnp.concatenate(rope, axis=0).astype(bf)
        kk = jnp.dot(lhs, wk[...], preferred_element_type=f32).astype(bf)
        vt = nt_dot(wvt[...], lhs).astype(bf)
        def scores(p):
            k2 = jnp.concatenate([kk[:, p * LANES:(p + 1) * LANES], rope], axis=1)
            s_buf[p] = jnp.dot(k2, q2t[p], preferred_element_type=f32)

        scores(0)
        for p in range(HC // 2):
            if p + 1 < HC // 2:
                scores(p + 1)
            old = m_sc[p:p + 1, :]
            new = jnp.maximum(old, jnp.max(s_buf[p], axis=0, keepdims=True))
            factor = jnp.exp2(old - new)
            m_sc[p:p + 1, :] = new
            expo = jnp.exp2(s_buf[p] - new)
            l_sc[p:p + 1, :] = l_sc[p:p + 1, :] * factor + jnp.sum(expo, axis=0, keepdims=True)
            weights_t = expo.astype(bf)
            for hh in range(2):
                h = 2 * p + hh
                lanes = slice(hh * 2 * T, (hh + 1) * 2 * T)
                o_sc[h] = o_sc[h] * factor[:, lanes] + jnp.dot(
                    vt[h * VALUE:(h + 1) * VALUE, :], weights_t[:, lanes], preferred_element_type=f32
                )

    base = served[0]
    rounds = HALF // 2
    turn = ZW[0] * min(AHEAD + 1, HALF)

    def phase(u, carry):
        for s in range(2):
            t = 2 * u + 1 + s
            pl.when(t + begun <= HALF)(lambda: lz_step(t + begun))
            k = base + t - 1
            pl.when(k < turn)(lambda: w_serve(0, k))
            pl.when(k >= turn)(lambda: w_serve(1, jnp.maximum(k - turn, 0)))
            if paired and s == 1:
                y_serve(0, u + 1)
            if s == 0:
                pl.when(u == min(1, rounds - 1))(lambda: x_relay(2))
            else:
                pl.when(u == min(2, rounds - 1))(lambda: x_share(2))

            ld_wait(t)
            attend(at(z - lax.rem(t, HALF)), at(z + t))
        return carry

    lax.fori_loop(0, rounds, phase, 0)
    served[0] = base + HALF
    y_done[0] = rounds

    heads = []
    for h in range(HC):
        p, hh = h // 2, h % 2
        heads.append(o_sc[h] / l_sc[p:p + 1, hh * 2 * T:(hh + 1) * 2 * T])
    final = m_sc[...] + jnp.log2(l_sc[...])
    for cc in range(2):
        lse[cc] = jnp.concatenate(
            [
                final[h // 2:h // 2 + 1, (2 * (h % 2) + cc) * T:(2 * (h % 2) + cc + 1) * T]
                for h in range(HC)
            ],
            axis=0,
        )
    here = 2 * x + c

    def owner(d, core):
        return {"sp": 2 * z + core, "tp": xat(d)}

    level = [
        rcopy(lse.at[cc], lrx.at[here], ml_s.at[0], ml_r.at[0], owner(d, cc)) for d in range(1, X) for cc in range(2)
    ]
    level.append(rcopy(lse.at[1 - c], lrx.at[here], ml_s.at[0], ml_r.at[0], sib))
    for copy in level:
        copy.start()
    lrx[here] = lse[c]
    ours = jnp.transpose(jnp.concatenate(heads, axis=0)).astype(bf)
    for q in range(X):
        for cc in range(2):
            obuf[q, cc] = ours[cc * T + q * share:cc * T + (q + 1) * share]
    far = [rcopy(obuf.at[xat(2), i], relay.at[i], mh_s.at[i], mh_r.at[i], xdev(d)) for i, d in enumerate((1, -1))]
    near = [
        rcopy(obuf.at[xat(d), cc], orx.at[here], mo_s.at[0], mo_r.at[0], owner(d, cc))
        for d in (1, -1) for cc in range(2)
    ]
    near.append(rcopy(obuf.at[x, 1 - c], orx.at[here], mo_s.at[0], mo_r.at[0], sib))
    for copy in far + near:
        copy.start()
    orx[here] = obuf[x, c]
    serve(4)
    for i, d in enumerate((1, -1)):
        far[i].wait_recv()
        rcopy(relay.at[i], orx.at[2 * xat(-d) + c], mo_s.at[0], mo_r.at[0], owner(d, i)).start()
    others = 2 * X - 1

    def seven(ref, ss, rs):
        return rcopy(ref.at[pl.ds(0, others)], ref.at[pl.ds(0, others)], ss.at[0], rs.at[0], sib)

    seven(lrx, ml_s, ml_r).wait_recv()
    coefs = []
    for core in range(2):
        levels = [lrx[2 * q + core] for q in range(X)]
        top = functools.reduce(jnp.maximum, levels)
        parts = [jnp.exp2(level_of - top) for level_of in levels]
        norm = 1.0 / functools.reduce(jnp.add, parts)
        coefs += [part_of * norm for part_of in parts]
    wts[...] = jnp.transpose(jnp.concatenate(coefs, axis=0))
    x_end(2)
    serve(4)
    need_y(0, HALF - 3)
    seven(orx, mo_s, mo_r).wait_recv()
    columns = wts[rowsof(x), :]
    for core in range(2):
        total = 0.0
        for q in range(X):
            first = (core * X + q) * HC
            coef = jnp.concatenate(
                [jnp.broadcast_to(columns[:, first + h:first + h + 1], (share, VALUE)) for h in range(HC)], axis=1
            )
            total = total + coef * orx[2 * q + core].astype(f32)
        mixed[:, core * HC * VALUE:(core + 1) * HC * VALUE] = total.astype(bf)
    NB = 256
    for n in range(W // NB):
        cols = slice(n * NB, (n + 1) * NB)
        branch = 0.0
        for q in range(X):
            rows = HP * VALUE
            branch = branch + jnp.dot(
                mixed[:, q * rows:(q + 1) * rows], WO[q, :, cols], preferred_element_type=f32
            )
        mid[:, cols] = (hrow[:, cols].astype(f32) + branch).astype(bf)
    nb[rowsof(x), :] = normalize(mid[...], gain)
    def quarter_rows(q, i):
        return nb.at[pl.ds(pl.multiple_of(q * share + i * (share // 2), share // 2), share // 2)]

    def spread_copy(n, i, d):
        piece = quarter_rows(x, i if n == 0 else 1 - i)
        return rcopy(piece, piece, ag_s.at[n, i], ag_r.at[n, i], xdev(d))

    spread = [[spread_copy(n, i, d) for i, d in enumerate((1, -1))] for n in range(2)]
    for copy in spread[0] + spread[1]:
        copy.start()
    need_y(0, HALF - 2)
    serve(5)
    onward = []
    for i, d in enumerate((1, -1)):
        spread[0][i].wait_recv()
        piece = quarter_rows(xat(-d), i)
        onward.append(rcopy(piece, piece, ah_s.at[i], ah_r.at[i], xdev(d)))
        onward[-1].start()
    serve(4)
    need_y(0, HALF - 1)
    serve(1)
    for copy in spread[1] + onward:
        copy.wait_recv()

    def wd_wait(arr, hop, count):
        rcopy(w_rows(count), w_rows(count), w_s.at[1], wd_r.at[0 if arr == 0 else hop], sib).wait_recv()

    serve_until(0, HALF)
    need_y(0, HALF)
    wd_wait(0, 0, Z * shard)
    CUTS = 4
    per = F // NB // CUTS
    for stage in range(CUTS):
        def up(n, carry):
            cols = pl.ds(pl.multiple_of(n * NB, NB), NB)
            high = jnp.maximum(jnp.dot(nb[...], U[:, cols], preferred_element_type=f32), 0.0)
            act[:, cols] = (high * high).astype(bf)
            return carry
        lax.fori_loop(stage * per, (stage + 1) * per, up, 0)
        if stage < CUTS - 1:
            serve(1)

    def fa_copy(t, i, d):
        return rcopy(osend.at[t, xat(2), i], opart.at[t, i], fa_s.at[0], fa_r.at[t], xdev(d))

    def fo_copy(t, i, d):
        return rcopy(osend.at[t, xat(d)], orecv.at[t, i], fo_s.at[0], fo_r.at[0], xdev(d))

    LAG = 3
    direct = rcopy(osend.at[HALF - 1, xat(2)], ofar, fz_s.at[0], fz_r.at[0], xdev(2))

    def pair_of(t):
        return at(z - (t % HALF)), at(z + t)

    def pass_on(t):
        rcopy(opart.at[t], opart.at[t], fa_s.at[0], fa_r.at[t], sib).wait_recv()
        for i, d in enumerate((1, -1)):
            osend[t, xat(d), i] = (osend[t, xat(d), i].astype(f32) + opart[t, i].astype(f32)).astype(bf)
            fo_copy(t, i, d).start()

    for t in range(1, HALF + 1):
        if 1 < t <= HALF // 2:
            serve(1)
        serve_until(1, t + 1)
        need_y(1, t)
        wd_wait(1, t, 2 * shard)
        rhs = jnp.concatenate(
            [D[pl.ds(pl.multiple_of(zz * 2 * shard, 2 * shard), 2 * shard), :] for zz in pair_of(t)], axis=0
        )
        block = nt_dot(act[...], rhs).astype(bf)
        for q in range(X):
            for side in range(2):
                osend[t - 1, q, side] = block[q * share:(q + 1) * share, side * LANES:(side + 1) * LANES]
        if t < HALF:
            for i, d in enumerate((1, -1)):
                fa_copy(t - 1, i, d).start()
        else:
            direct.start()
            for i, d in enumerate((1, -1)):
                fo_copy(t - 1, i, d).start()
        if t > LAG:
            pass_on(t - 1 - LAG)
    for t in range(max(HALF - LAG, 0), HALF - 1):
        pass_on(t)
    rcopy(orecv, orecv, fo_s.at[0], fo_r.at[0], sib).wait_recv()
    direct.wait_recv()
    for t in range(1, HALF + 1):
        for side, zz in enumerate(pair_of(t)):
            cols = pl.ds(pl.multiple_of(zz * LANES, LANES), LANES)
            total = osend[t - 1, x, side].astype(f32)
            for i in range(2):
                total = total + orecv[t - 1, i, side].astype(f32)
            if t == HALF:
                total = total + ofar[side].astype(f32)
            out[:, cols] = (mid[:, cols].astype(f32) + total).astype(bf)

    for copy in far + spread[0] + spread[1] + onward + [direct]:
        copy.wait_send()
    seven(lrx, ml_s, ml_r).wait_send()
    seven(orx, mo_s, mo_r).wait_send()
    sent = opart.at[pl.ds(0, HALF - 1)]
    rcopy(sent, sent, fa_s.at[0], fa_r.at[0], sib).wait_send()
    rcopy(orecv, orecv, fo_s.at[0], fo_r.at[0], sib).wait_send()
    for what in range(3):
        for i, d in enumerate((1, -1)):
            x1_copy(what, i, d).wait_send()
            x2_copy(what, i, d).wait_send()
        for n in range(X - 1 if what == 2 else X // 2):
            if what == 0:
                pl.when((1 - c) * (X // 2) + n != x)(lambda: xd_copy(0, n).wait_send())
            else:
                xd_copy(what, n).wait_send()
    sent = xb.at[pl.ds(0, Z - 1), 0]
    rcopy(sent, sent, lz_s.at[0], lz_r.at[0, 0], sib).wait_send()
    sent = xb.at[pl.ds(0, HALF)]
    rcopy(sent, sent, ld_s.at[0], ld_r.at[0], sib).wait_send()
    sent = w_rows(2 * (Z - 1) * 4 * part)
    rcopy(sent, sent, w_s.at[0], wz_r.at[0, 0], sib).wait_send()
    sent = w_rows(2 * Z * shard)
    rcopy(sent, sent, w_s.at[1], wd_r.at[0], sib).wait_send()


def fused_layer(Z, X, paired, kvl, key_t, up_own, dn_own, hid, ql, wq, wkv, wo, cos_t, sin_t, q_gain, kv_gain, gain):
    HALF = Z // 2
    T, W = hid.shape
    F = up_own.shape[1]
    share = T // X
    rows = kvl.shape[1] // LANES * share + share * ROTARY // LANES
    bf, f32 = jnp.bfloat16, jnp.float32
    DMA = pltpu.SemaphoreType.DMA
    any_ = pl.BlockSpec(memory_space=pl.ANY)
    vm = pl.BlockSpec(memory_space=pltpu.VMEM)
    R = kvl.shape[1]
    hc = wkv.shape[1] // (PLAIN + VALUE) * X // 2
    scratch = [
        pltpu.VMEM((Z, 2, rows, LANES), bf),
        pltpu.VMEM((T, LANES), f32),
        pltpu.VMEM((W, F), bf),
        pltpu.VMEM((W, F), bf),
        pltpu.VMEM((share, W), bf),
        pltpu.VMEM((X,) + wkv.shape, bf),
        pltpu.VMEM((X,) + wo.shape, bf),
        pltpu.VMEM((X, 2, wq.shape[1], T), bf),
        pltpu.VMEM((hc // 2, 2 * LANES, 4 * T), bf),
        pltpu.VMEM((R, hc * PLAIN), bf),
        pltpu.VMEM((hc * VALUE, R), bf),
        pltpu.VMEM((hc // 2, 4 * share, 4 * T), f32),
        pltpu.VMEM((hc // 2, 4 * T), f32),
        pltpu.VMEM((hc // 2, 4 * T), f32),
        pltpu.VMEM((hc, VALUE, 2 * T), f32),
        pltpu.VMEM((X, 2, share, hc * VALUE), bf),
        pltpu.VMEM((X * 2, share, hc * VALUE), bf),
        pltpu.VMEM((2, share, hc * VALUE), bf),
        pltpu.VMEM((2, hc, T), f32),
        pltpu.VMEM((X * 2, hc, T), f32),
        pltpu.VMEM((T, X * 2 * hc), f32),
        pltpu.VMEM((share, 2 * hc * VALUE), bf),
        pltpu.VMEM((share, W), bf),
        pltpu.VMEM((T, W), bf),
        pltpu.VMEM((T, F), bf),
        pltpu.VMEM((HALF, X, 2, share, LANES), bf),
        pltpu.VMEM((HALF, 2, 2, share, LANES), bf),
        pltpu.VMEM((HALF, 2, share, LANES), bf),
        pltpu.VMEM((2, share, LANES), bf),
        DMA((5,)),
    ]
    for shape in (
        (1,), (2, HALF + 1), (1,), (HALF + 1,),
        (2,), (2, 4 * HALF), (2, HALF + 1), (HALF + 1,),
        (3, 2), (3, 2), (3, 2), (3, 2), (3, X - 1), (3, X - 1), (1,), (1,), (1,), (1,), (2,), (2,),
        (2, 2), (2, 2), (2,), (2,), (1,), (HALF,), (1,), (1,), (1,), (1,),
    ):
        scratch.append(DMA(shape))
    return pl.pallas_call(
        functools.partial(layer_kernel, Z, X, paired),
        out_shape=jax.ShapeDtypeStruct((share, W), bf),
        in_specs=[vm, vm, any_, any_, any_, vm, vm, any_, any_] + [vm] * 5,
        out_specs=vm,
        scratch_shapes=scratch,
        compiler_params=pltpu.CompilerParams(
            collective_id=0, has_side_effects=True, vmem_limit_bytes=62 * 1024 * 1024
        ),
        name="layer",
    )(kvl, key_t, up_own, dn_own, hid, ql, wq, wkv, wo, cos_t, sin_t, q_gain, kv_gain, gain)


def on_device(
    hidden_in, query_latent_rows, key_value_latent, rotary_key, query_norm_gain, key_value_gain,
    query_up_weight, key_value_up_weight, out_proj, feed_gain, feed_up, feed_down,
):
    X = lax.axis_size("tp")
    Z = lax.axis_size("sp") // 2
    paired = lax.axis_size("grp") % 2 == 0
    T = hidden_in.shape[0]
    half = ROTARY // 2
    position = (lax.axis_index("sp") * T + jnp.arange(T)).astype(jnp.float32)
    inverse = 10000.0 ** (-jnp.arange(half, dtype=jnp.float32) * 2.0 / ROTARY)
    angles = inverse[:, None] * position[None, :]
    return fused_layer(
        Z, X, paired, key_value_latent, rotary_key.T, feed_up, feed_down.T, hidden_in, query_latent_rows,
        query_up_weight, key_value_up_weight, out_proj, jnp.cos(angles), jnp.sin(angles),
        query_norm_gain.reshape(-1, LANES), key_value_gain.reshape(-1, LANES), feed_gain.reshape(-1, LANES),
    )


def solution(mesh):
    return jax.shard_map(
        on_device,
        mesh=mesh,
        in_specs=(
            P(("grp", "sp"), None),
            P(("grp", "sp"), None),
            P(("grp", "sp"), None),
            P(("grp", "sp"), None),
            P(),
            P(),
            P(None, "tp"),
            P(None, "tp"),
            P("tp", None),
            P(),
            P("sp", "tp"),
            P("tp", "sp"),
        ),
        out_specs=P(("grp", "sp", "tp"), None),
        check_vma=False,
    )
```
